32 devices in a mesh: grp: 2 (over y), sp: 4 (over z), tp: 4 (over x, core).
Axes of the slice: x: 2, y: 2, z: 4, core: 2. Of those that a mesh axis runs over, the one named last changes fastest.
Arguments:
- stream: bfloat16 [2048, 2048], P(('grp', 'sp')), parts along dimension 0, may hold values from -6 to 6
- doc_ids: int32 [2048], P(('grp', 'sp')), parts along dimension 0, may hold values from 0 to 1, never falling along the last dimension, each value on 1 to 768 neighbouring positions
- norm_gain: float32 [2, 2048], replicated, may hold values from 0.1 to 1.9
- query_weight: bfloat16 [2, 2048, 1024], P(None, 'sp', 'tp'), may hold values from -0.125 to 0.125
- key_weight: bfloat16 [2, 2048, 1024], P(None, 'sp', 'tp'), may hold values from -0.125 to 0.125
- value_weight: bfloat16 [2, 2048, 1024], P(None, 'sp', 'tp'), may hold values from -0.125 to 0.125
- out_weight: bfloat16 [2, 1024, 2048], P(None, 'sp', 'tp'), may hold values from -0.75 to 0.75
- query_gain: float32 [2, 64], replicated, may hold values from 0.1 to 1.9
- key_gain: float32 [2, 64], replicated, may hold values from 0.1 to 1.9
- rel_bias: float32 [16, 513], P('tp'), may hold values from -4 to 250
Outputs:
- encoded: bfloat16 [2048, 2048], P(('grp', 'sp')), parts along dimension 0
The draws below stay inside these ranges and needn't reach their ends.
There are 2 independent parts, one for each index of `grp`. The reference program is written for one: setup_inputs(seed, part) draws one part's arguments, and reference() takes and returns one part's arrays. A program takes and returns all parts, laid end to end along the dimension named above; an argument that names none is the same for every part. Nothing has to cross between parts.
Inputs may be any that keep to these rules, and one draw needn't show every extreme that they name: doc_ids never fall along the sequence; each document has at most 768 positions.
All inputs are finite; a program needn't handle non-finite values.
Results may differ from the reference program's by a relative error of at most 0.011.
Values may be sent and summed in bfloat16 or wider, within the bound.
A program may use at most 64 MiB of HBM per device.

```python
import math
import jax
import jax.numpy as jnp
import numpy as np
from jax import lax

D = 2048
HEADS = 16
HD = 64
DA = 1024
SEG = 64
LEFT = 8
MAXREL = 256
NREL = 513
LAYERS = 2
TOK_DEV = 256
TOKENS = 1024
DOCS = 2


def draw_rel_bias(key, part):
    base_key = jax.random.fold_in(key, 11)
    table = jnp.clip(jax.random.normal(base_key, (HEADS, NREL), jnp.float32), -4.0, 4.0)
    return table


def block_scale(rng, extent, shards, least, high):
    def one(position, blocks):
        heights = jax.random.uniform(jax.random.fold_in(jax.random.fold_in(rng, 6), position), (blocks,), jnp.float32, least / len(shards), high / len(shards))
        return jnp.repeat(jnp.exp(heights), extent[position] // blocks).reshape((-1,) + (1,) * (len(extent) - position - 1))

    level = one(*shards[0])
    for cut in shards[1:]:
        level = level * one(*cut)
    return level


def profile(amount, total, most, skew):
    weights = [(1 << 20) // math.isqrt(standing ** skew) + 1 for standing in range(2, amount + 1)]
    rest, holding = total - most - (amount - 1), [1] * (amount - 1)
    while rest > 0:
        candidates = [i for i in range(amount - 1) if holding[i] < most]
        whole, left = sum([weights[i] for i in candidates]), rest
        for i in candidates:
            extra = min(most - holding[i], max(1, left * weights[i] // whole), rest)
            holding[i] = holding[i] + extra
            rest = rest - extra
    return np.array([most] + holding)


def uneven_parts(own_key, count, total, bound, lean):
    if count == 2:
        one = jax.random.randint(own_key, (), max(1, total - bound), min(bound, total - 1) + 1)
        return jnp.stack([one, total - one])
    tallies = jnp.asarray(profile(count, total, bound, lean), jnp.int32)
    couples = (count - 1) // 2
    giver, taker = tallies[1:1 + 2 * couples:2], tallies[2:2 + 2 * couples:2]
    slack = jnp.minimum(giver - 1, bound - taker)
    shifted = jax.random.randint(jax.random.fold_in(own_key, 1), (couples,), 0, 1 << 20) % (slack + 1)
    tallies = tallies.at[1:1 + 2 * couples:2].set(giver - shifted).at[2:2 + 2 * couples:2].set(taker + shifted)
    return tallies[jax.random.permutation(jax.random.fold_in(own_key, 2), count)]


def noise(key, shape, scale, most, cuts=(), kind=jnp.bfloat16):
    values = scale * jax.random.normal(key, shape, jnp.float32)
    if cuts:
        values = values * block_scale(key, shape, cuts, -0.22, 0.18)
    return jnp.clip(values, -most, most).astype(kind)


def setup_inputs(seed: int = 0, part: int = 0) -> dict:
    key_of = jax.random.split(jax.random.key(seed), 11)
    part_splits = jax.random.split(jax.random.fold_in(key_of[10], part), 11)
    stream = noise(part_splits[0], (TOKENS, D), 1.0, 6.0, ((0, 4),))
    doc_ids = jnp.searchsorted(jnp.cumsum(uneven_parts(part_splits[1], DOCS, TOKENS, 3 * TOK_DEV, 1)), jnp.arange(TOKENS), side="right").astype(jnp.int32)
    norm_gain = jnp.clip(1.0 + 0.18 * jax.random.normal(key_of[2], (LAYERS, D), jnp.float32), 0.1, 1.9)
    query_weight = noise(key_of[3], (LAYERS, D, DA), D ** -0.5, 0.125, ((1, 4), (2, 4)))
    key_weight = noise(key_of[4], (LAYERS, D, DA), D ** -0.5, 0.125, ((1, 4), (2, 4)))
    value_weight = noise(key_of[5], (LAYERS, D, DA), D ** -0.5, 0.125, ((1, 4), (2, 4)))
    out_weight = noise(key_of[6], (LAYERS, DA, D), (DA // 16) ** -0.5, 0.75, ((1, 4), (2, 4)))
    query_gain = jnp.clip(1.0 + 0.18 * jax.random.normal(key_of[7], (LAYERS, HD), jnp.float32), 0.1, 1.9)
    key_gain = jnp.clip(1.0 + 0.18 * jax.random.normal(key_of[8], (LAYERS, HD), jnp.float32), 0.1, 1.9)
    rel_bias = draw_rel_bias(jax.random.fold_in(key_of[10], 71), part)
    return {"stream": stream, "doc_ids": doc_ids, "norm_gain": norm_gain, "query_weight": query_weight, "key_weight": key_weight, "value_weight": value_weight, "out_weight": out_weight, "query_gain": query_gain, "key_gain": key_gain, "rel_bias": rel_bias}


epsilon = 1e-06

def row_norm(values, gain):
    return values * lax.rsqrt(lax.optimization_barrier(jnp.mean(values * values, axis=-1, keepdims=True)) + epsilon) * gain

def band_of(values, count):
    blocks = values.reshape((count + LEFT, SEG) + values.shape[1:])
    stacked = jnp.stack([blocks[earlier:earlier + count] for earlier in range(LEFT + 1)], axis=1)
    return stacked.reshape((count, (LEFT + 1) * SEG) + values.shape[1:])

def reference(stream, doc_ids, norm_gain, query_weight, key_weight, value_weight, out_weight, query_gain, key_gain, rel_bias):
    total = stream.shape[0]
    count = total // SEG
    reach = LEFT * SEG
    width = (LEFT + 1) * SEG
    scale = HD ** (-0.5)
    distance = reach + jnp.arange(SEG, dtype=jnp.int32)[:, None] - jnp.arange(width, dtype=jnp.int32)[None, :]
    index = (jnp.clip(distance, -MAXREL, MAXREL) + MAXREL).astype(jnp.int32)
    table = jnp.take(rel_bias.astype(jnp.float32), index, axis=1)
    padded_docs = jnp.concatenate([jnp.full((reach,), -1, jnp.int32), doc_ids.astype(jnp.int32)])
    doc_band = band_of(padded_docs, count)
    key_pos = SEG * jnp.arange(count, dtype=jnp.int32)[:, None] - reach + jnp.arange(width, dtype=jnp.int32)[None, :]
    allowed = (key_pos >= 0)[:, None, :] & (doc_band[:, None, :] == doc_ids.reshape(count, SEG)[:, :, None])
    x = stream
    for layer in range(LAYERS):
        widened = x.astype(jnp.float32)
        normed = row_norm(widened, norm_gain[layer]).astype(jnp.bfloat16)
        q_raw = jnp.dot(normed, query_weight[layer], preferred_element_type=jnp.float32).reshape(total, HEADS, HD)
        k_raw = jnp.dot(normed, key_weight[layer], preferred_element_type=jnp.float32).reshape(total, HEADS, HD)
        v_raw = jnp.dot(normed, value_weight[layer], preferred_element_type=jnp.float32).reshape(total, HEADS, HD)
        query = row_norm(q_raw, query_gain[layer]).astype(jnp.bfloat16)
        keys = row_norm(k_raw, key_gain[layer]).astype(jnp.bfloat16)
        values = v_raw.astype(jnp.bfloat16)

        def one_head(operands):
            head_query, head_keys, head_values, head_table = operands
            pad_keys = jnp.concatenate([jnp.zeros((reach, HD), jnp.bfloat16), head_keys], axis=0)
            pad_values = jnp.concatenate([jnp.zeros((reach, HD), jnp.bfloat16), head_values], axis=0)
            key_band = band_of(pad_keys, count).astype(jnp.float32)
            value_band = band_of(pad_values, count).astype(jnp.float32)
            blocks = head_query.reshape(count, SEG, HD).astype(jnp.float32)
            scores = jnp.einsum('nqd,nkd->nqk', blocks, key_band) * scale + head_table[None]
            scores = jnp.where(allowed, scores, -1e+30)
            peak = lax.optimization_barrier(jnp.max(scores, axis=-1, keepdims=True))
            expo = jnp.exp(scores - peak)
            weights = (expo / lax.optimization_barrier(jnp.sum(expo, axis=-1, keepdims=True))).astype(jnp.bfloat16)
            mixed = jnp.einsum('nqk,nkd->nqd', weights.astype(jnp.float32), value_band)
            return mixed.astype(jnp.bfloat16).reshape(total, HD)
        attended = lax.map(one_head, (query.transpose(1, 0, 2), keys.transpose(1, 0, 2), values.transpose(1, 0, 2), table))
        attended = attended.transpose(1, 0, 2).reshape(total, HEADS * HD)
        x = (widened + jnp.dot(attended, out_weight[layer], preferred_element_type=jnp.float32)).astype(jnp.bfloat16)
    return x
```

```python
import functools

import jax
import jax.numpy as jnp
from jax import lax
from jax.experimental import pallas as pl
from jax.experimental.pallas import tpu as pltpu
from jax.sharding import PartitionSpec as P

SEG = 64
LEFT = 8
MAXREL = 256
LAYERS = 2


epsilon = 1e-06


def shifted(value, axis, steps):
    count = lax.axis_size(axis)
    initial, last = (max(0, -steps), min(count, count - steps))
    return lax.ppermute(value, axis, [(source, source + steps) for source in range(initial, last)])


def row_norm(values, gain):
    return values * lax.rsqrt(jnp.mean(values * values, axis=-1, keepdims=True) + epsilon) * gain


def bias_table(rel_bias):
    heads_here = rel_bias.shape[0]
    reach = LEFT * SEG
    width = (LEFT + 1) * SEG
    highest = reach + SEG - 1
    reversed_bias = rel_bias[:, ::-1]
    upper_fill = jnp.broadcast_to(rel_bias[:, -1:], (heads_here, highest - MAXREL))
    flat_row = jnp.concatenate([upper_fill, reversed_bias[:, : MAXREL + SEG]], axis=1)
    lines = [
        flat_row[:, SEG - 1 - position : SEG - 1 - position + width] for position in range(SEG)
    ]
    return jnp.stack(lines, axis=1)


def attend(query, ext_keys, ext_values, ext_docs, own_docs, offset, table):
    rows, heads_here, head_size = query.shape
    count = rows // SEG
    width = (LEFT + 1) * SEG
    blocks = query.reshape(count, SEG, heads_here, head_size)
    key_blocks = ext_keys.reshape(count + LEFT, SEG, heads_here, head_size)
    value_blocks = ext_values.reshape(count + LEFT, SEG, heads_here, head_size)
    doc_blocks = ext_docs.reshape(count + LEFT, SEG)
    score_parts = [
        jnp.einsum(
            "nqhd,nkhd->nhqk",
            blocks,
            key_blocks[earlier : earlier + count],
            preferred_element_type=jnp.float32,
        )
        for earlier in range(LEFT + 1)
    ]
    scores = jnp.concatenate(score_parts, axis=-1)
    scores = scores * head_size ** (-0.5) + table[None]
    doc_band = jnp.concatenate(
        [doc_blocks[earlier : earlier + count] for earlier in range(LEFT + 1)], axis=1
    )
    key_pos = (
        offset
        + SEG * jnp.arange(count, dtype=jnp.int32)[:, None]
        - LEFT * SEG
        + jnp.arange(width, dtype=jnp.int32)[None, :]
    )
    allowed = (key_pos >= 0)[:, None, None, :] & (
        doc_band[:, None, None, :] == own_docs.reshape(count, SEG)[:, None, :, None]
    )
    scores = jnp.where(allowed, scores, -1e30)
    peak = jnp.max(scores, axis=-1, keepdims=True)
    expo = jnp.exp(scores - peak)
    weights = (expo / jnp.sum(expo, axis=-1, keepdims=True)).astype(jnp.bfloat16)
    mixed = jnp.zeros((count, SEG, heads_here, head_size), jnp.float32)
    for earlier in range(LEFT + 1):
        part_weights = weights[..., earlier * SEG : (earlier + 1) * SEG]
        mixed = mixed + jnp.einsum(
            "nhqk,nkhd->nqhd",
            part_weights,
            value_blocks[earlier : earlier + count],
            preferred_element_type=jnp.float32,
        )
    return mixed.astype(jnp.bfloat16).reshape(rows, heads_here * head_size)


def on_device(
    stream,
    doc_ids,
    norm_gain,
    query_weight,
    key_weight,
    value_weight,
    out_weight,
    query_gain,
    key_gain,
    rel_bias,
):
    rows = stream.shape[0]
    heads_here = rel_bias.shape[0]
    head_size = query_gain.shape[1]
    local_width = heads_here * head_size
    reach = LEFT * SEG
    depth = -(-reach // rows)
    offset = lax.axis_index("sp") * rows
    col_width = out_weight.shape[2]
    col_start = lax.axis_index("tp") * col_width
    table = bias_table(rel_bias)
    x = stream
    for layer in range(LAYERS):
        widened = x.astype(jnp.float32)
        normed = row_norm(widened, norm_gain[layer]).astype(jnp.bfloat16)
        own_cols = normed
        q_raw = jnp.dot(
            own_cols,
            lax.all_gather(query_weight[layer], "sp", axis=0, tiled=True),
            preferred_element_type=jnp.float32,
        )
        k_raw = jnp.dot(
            normed,
            lax.all_gather(key_weight[layer], "sp", axis=0, tiled=True),
            preferred_element_type=jnp.float32,
        )
        v_raw = jnp.dot(
            normed,
            lax.all_gather(value_weight[layer], "sp", axis=0, tiled=True),
            preferred_element_type=jnp.float32,
        )
        query = row_norm(q_raw.reshape(rows, heads_here, head_size), query_gain[layer]).astype(
            jnp.bfloat16
        )
        keys = row_norm(
            k_raw.reshape(normed.shape[0], heads_here, head_size), key_gain[layer]
        ).astype(jnp.bfloat16)
        values = v_raw.astype(jnp.bfloat16)
        flat_keys = keys.reshape(rows, local_width)
        tail = (flat_keys, values, doc_ids)
        received = [
            shifted((tail[0], tail[1], tail[2]), "sp", distance_back)
            for distance_back in range(depth, 0, -1)
        ]
        ext_keys = jnp.concatenate([item[0] for item in received] + [flat_keys], axis=0)
        ext_values = jnp.concatenate([item[1] for item in received] + [values], axis=0)
        ext_docs = jnp.concatenate([item[2] for item in received] + [doc_ids], axis=0)
        ext_keys = ext_keys.reshape(reach + rows, heads_here, head_size)
        ext_values = ext_values.reshape(reach + rows, heads_here, head_size)
        attended = attend(query, ext_keys, ext_values, ext_docs, doc_ids, offset, table)
        all_heads = lax.all_gather(attended, "tp", axis=1, tiled=True)
        projected = jnp.dot(
            all_heads,
            lax.all_gather(out_weight[layer], "sp", axis=0, tiled=True),
            preferred_element_type=jnp.float32,
        )
        own_cols = lax.dynamic_slice_in_dim(widened, col_start, col_width, 1)
        new_cols = (own_cols + projected).astype(jnp.bfloat16)
        x = lax.all_gather(new_cols, "tp", axis=1, tiled=True)
    return x


MESH = pl.DeviceIdType.MESH
NEG = -1e30


def fused_kernel(
    sizes,
    x_ref,
    docs_ref,
    ngain_ref,
    qw_ref,
    kw_ref,
    vw_ref,
    woin_ref,
    qgain_ref,
    kgain_ref,
    bias_ref,
    out_ref,
    wt_ref,
    xg,
    wq,
    wo,
    docs,
    dcol,
    mids,
    ag,
    fin,
    bias,
    nb,
    q_s,
    k_s,
    v_s,
    o_s,
    doc_send,
    doc_recv,
    xz_send,
    xz_recv,
    xt_send,
    xt_recv,
    wz_send,
    wz_recv,
    wy_send,
    wy_recv,
    oz_send,
    oz_recv,
    ox_send,
    ox_recv,
    oy_send,
    oy_recv,
    op_send,
    op_recv,
    mz_send,
    mz_recv,
    mx_send,
    mx_recv,
    mc_send,
    mc_recv,
    nc_send,
    nc_recv,
    az_send,
    az_recv,
    at_send,
    at_recv,
    fn_send,
    fn_recv,
):
    groups, seqs, tps = sizes
    rows, width = x_ref.shape
    cols = width // tps
    head = qgain_ref.shape[1]
    layers = wt_ref.shape[0]
    depth = bias.shape[0] - 1
    grp = lax.axis_index("grp")
    s = lax.axis_index("sp")
    t = lax.axis_index("tp")
    other_grp = 1 - grp
    core = t + 1 - 2 * lax.rem(t, 2)
    side = lax.rem(t + 2, tps)
    started = []

    def send(src, dst, sems, index, where):
        copy = pltpu.make_async_remote_copy(
            src_ref=src,
            dst_ref=dst,
            send_sem=sems[0].at[index],
            recv_sem=sems[1].at[index],
            device_id=where,
            device_id_type=MESH,
        )
        copy.start()
        started.append(copy)
        return copy

    def ahead(o):
        return lax.rem(s + o, seqs)

    def behind(o):
        return lax.rem(s + seqs - o, seqs)

    def block_rows(i):
        return pl.ds(pl.multiple_of(i * rows, rows), rows)

    barrier = pltpu.get_barrier_semaphore()
    partners = [{"sp": ahead(o)} for o in range(1, seqs)]
    partners += [{"tp": core}, {"tp": side}, {"grp": other_grp}]
    for where in partners:
        pl.semaphore_signal(barrier, inc=1, device_id=where, device_id_type=MESH)
    pl.semaphore_wait(barrier, len(partners))

    own_cols = pl.ds(pl.multiple_of(t * cols, cols), cols)
    whalf = wt_ref.shape[2] // 2
    ohalf = woin_ref.shape[1] // 2
    wpart = pl.ds(pl.multiple_of(grp * whalf, whalf), whalf)
    opart = pl.ds(pl.multiple_of(grp * ohalf, ohalf), ohalf)
    hops = list(range(1, seqs))

    def passing(way, k, arriving):
        block = s - k if way == 0 else s + k
        if arriving:
            block = block - 1 if way == 0 else block + 1
        inside = block >= 0 if way == 0 else block < seqs
        return block, inside

    def onward(way, k):
        block, inside = passing(way, k, False)
        open_end = s < seqs - 1 if way == 0 else s > 0
        place = xg.at[0, t, block_rows(block), :]
        copy = pltpu.make_async_remote_copy(
            src_ref=x_ref.at[:, own_cols] if k == 0 else place,
            dst_ref=place,
            send_sem=xz_send.at[way, k],
            recv_sem=xz_recv.at[way, k],
            device_id={"sp": s + 1 if way == 0 else s - 1},
            device_id_type=MESH,
        )
        return copy, inside & open_end

    def start_onward(way, k):
        copy, valid = onward(way, k)

        @pl.when(valid)
        def _():
            copy.start()

    def tp_copy(kind, block):
        held = side if kind == 2 else t
        place = xg.at[0, held, block_rows(block), :]
        return pltpu.make_async_remote_copy(
            src_ref=place,
            dst_ref=place,
            send_sem=xt_send.at[kind, block],
            recv_sem=xt_recv.at[kind, block],
            device_id={"tp": side if kind == 1 else core},
            device_id_type=MESH,
        )

    def fan(block):
        tp_copy(1, block).start()
        tp_copy(0, block).start()

    def pass_slots(k):
        for way in (0, 1):
            block, inside = passing(way, k, True)

            @pl.when(inside)
            def _(block=block):
                tp_copy(1, block).wait_recv()
                tp_copy(2, block).start()

    for way in (0, 1):
        start_onward(way, 0)
    doc_c = [
        send(docs_ref, docs.at[s], (doc_send, doc_recv), o, {"sp": ahead(o)}) for o in hops
    ]

    def send_qkv(layer):
        return {
            o: send(
                wt_ref.at[layer, ahead(o), wpart, :],
                wq.at[layer, s, wpart, :],
                (wz_send, wz_recv),
                (layer, o),
                {"sp": ahead(o)},
            )
            for o in hops
        }

    def relay_qkv(layer, flying):
        result = []
        for o in hops:
            flying[o].wait_recv()
            block = wq.at[layer, behind(o), wpart, :]
            result.append(send(block, block, (wy_send, wy_recv), (layer, o), {"grp": other_grp}))
        return result

    def send_out(layer):
        flying = {
            o: send(
                woin_ref.at[layer, opart, :],
                wo.at[layer, t, s, opart, :],
                (oz_send, oz_recv),
                (layer, o),
                {"sp": ahead(o)},
            )
            for o in hops
        }
        whole = send(
            woin_ref.at[layer], wo.at[layer, t, s], (ox_send, ox_recv), (layer, 0), {"tp": side}
        )
        return flying, whole

    def relay_out(layer, flying):
        across, over = {}, []
        for o in hops:
            flying[o].wait_recv()
            block = wo.at[layer, t, behind(o), opart, :]
            across[o] = send(block, block, (ox_send, ox_recv), (layer, o), {"tp": side})
            over.append(send(block, block, (oy_send, oy_recv), (layer, o), {"grp": other_grp}))
        return across, over

    def relay_side(layer, across, over):
        for o in hops:
            across[o].wait_recv()
            block = wo.at[layer, side, behind(o), opart, :]
            over.append(send(block, block, (op_send, op_recv), (layer, o), {"grp": other_grp}))

    def turn(layer):
        for which, source in enumerate((qw_ref, kw_ref, vw_ref)):
            turned = jnp.transpose(source[layer])
            for i in range(seqs):
                wt_ref[layer, i, which * head : (which + 1) * head, :] = turned[
                    i * head : (i + 1) * head, :
                ]
        wq[layer, s] = wt_ref[layer, s]

    turn(0)
    qkv_fly = send_qkv(0)
    for part in range(tps):
        xg[0, part, block_rows(s), :] = x_ref[:, part * cols : (part + 1) * cols]
    for layer in range(1, layers):
        turn(layer)
    for layer in range(layers):
        wo[layer, t, s] = woin_ref[layer]
    docs[s] = docs_ref[...]
    key_seg = lax.broadcasted_iota(jnp.int32, (rows, rows), 0) // SEG
    query_seg = lax.broadcasted_iota(jnp.int32, (rows, rows), 1) // SEG
    for d in range(depth + 1):
        spread = jnp.broadcast_to(
            bias_ref[pl.ds(s, 1), d * rows : (d + 2) * rows], (rows, 2 * rows)
        )
        rolled = pltpu.roll(spread, 0, 1, stride=1, stride_axis=0)
        gap = query_seg + (d * rows) // SEG - key_seg
        bias[d] = jnp.where((gap >= 0) & (gap <= LEFT), rolled[:, rows:], NEG)
    for copy in doc_c:
        copy.wait_recv()
    for i in range(seqs):
        dcol[i] = jnp.transpose(jnp.broadcast_to(docs[i, 0:1, :], (128, rows)))

    for k in range(seqs - 1):
        for way in (0, 1):
            block, inside = passing(way, k, True)

            @pl.when(inside)
            def _(block=block, way=way, k=k):
                onward(way, k)[0].wait_recv()
                if k + 1 < seqs - 1:
                    start_onward(way, k + 1)
                fan(block)

        if k == 0:
            qkv_ready = relay_qkv(0, qkv_fly)
        else:
            pass_slots(k - 1)
    out_fly, out_whole = send_out(0)
    pass_slots(seqs - 2)

    def nth(v):
        orders = [
            sorted((b for b in range(seqs) if b != c), key=lambda b: abs(b - c))
            for c in range(seqs)
        ]
        block = orders[0][v - 1]
        for c in range(1, seqs):
            block = jnp.where(s == c, orders[c][v - 1], block)
        return block

    def project(layer, i):
        total = jnp.zeros((rows, 1), jnp.float32)
        for part in range(tps):
            piece = xg[layer, part, block_rows(i), :].astype(jnp.float32)
            total = total + jnp.sum(piece * piece, axis=1, keepdims=True)
        factor = lax.rsqrt(total * (1.0 / width) + epsilon)
        for part in range(tps):
            piece = xg[layer, part, block_rows(i), :].astype(jnp.float32)
            gain = ngain_ref[layer : layer + 1, part * cols : (part + 1) * cols]
            nb[:, part * cols : (part + 1) * cols] = (piece * factor * gain).astype(jnp.bfloat16)
        span = width // seqs
        raw = jnp.zeros((3 * head, rows), jnp.float32)
        for part in range(seqs):
            raw = raw + lax.dot_general(
                wq[layer, part],
                nb[:, part * span : (part + 1) * span],
                (((1,), (1,)), ((), ())),
                preferred_element_type=jnp.float32,
            )

        def normal(value, gain):
            mean = jnp.mean(value * value, axis=0, keepdims=True)
            column = jnp.transpose(jnp.broadcast_to(gain, (128, head)))[:, 0:1]
            return value * lax.rsqrt(mean + epsilon) * column

        q_s[i] = (normal(raw[:head], qgain_ref[layer : layer + 1, :]) * head ** (-0.5)).astype(jnp.bfloat16)
        k_s[i] = jnp.transpose(normal(raw[head : 2 * head], kgain_ref[layer : layer + 1, :])).astype(jnp.bfloat16)
        v_s[i] = raw[2 * head :].astype(jnp.bfloat16)

    def attend_block(j):
        pieces = []
        for i in range(max(0, j - depth), j + 1):
            score = jnp.dot(k_s[i], q_s[j], preferred_element_type=jnp.float32)
            same = dcol[i][:, 0:1] == docs[j, 0:1, :]
            pieces.append((i, jnp.where(same, score + bias[j - i], NEG)))
        peak = pieces[0][1].max(axis=0, keepdims=True)
        for _, piece in pieces[1:]:
            peak = jnp.maximum(peak, piece.max(axis=0, keepdims=True))
        mass = jnp.zeros((1, rows), jnp.float32)
        mixed = jnp.zeros((head, rows), jnp.float32)
        for i, piece in pieces:
            expo = jnp.exp(piece - peak)
            mass = mass + jnp.sum(expo, axis=0, keepdims=True)
            mixed = mixed + jnp.dot(
                v_s[i], expo.astype(jnp.bfloat16), preferred_element_type=jnp.float32
            )
        return (mixed / mass).astype(jnp.bfloat16)

    def out_product(layer, heads_all, held):
        return lax.dot_general(
            heads_all,
            wo[layer, held].reshape(-1, cols),
            (((0,), (0,)), ((), ())),
            preferred_element_type=jnp.float32,
        )

    for copy in qkv_ready:
        copy.wait_recv()
    for v in range(seqs):
        block = nth(v) if v else s
        if v:
            tp_copy(0, block).wait_recv()
            tp_copy(2, block).wait_recv()
        project(0, block)

    mid_z, mid_x, mid_c, new_c = {}, {}, {}, {}
    for j in range(seqs):
        mids[j, t, s] = attend_block(j)
        place = mids.at[j, t, s]
        for o in hops:
            mid_z[j, o] = send(place, place, (mz_send, mz_recv), (j, o), {"sp": ahead(o)})
        mid_x[j, 0] = send(place, place, (mx_send, mx_recv), (j, 0), {"tp": side})
    out_across, out_over = relay_out(0, out_fly)
    qkv_fly = send_qkv(1)

    def mid_first(j):
        for o in hops:
            mid_z[j, o].wait_recv()
            place = mids.at[j, t, behind(o)]
            mid_x[j, o] = send(place, place, (mx_send, mx_recv), (j, o), {"tp": side})
        place = mids.at[j, t]
        mid_c[j, 0] = send(place, place, (mc_send, mc_recv), (j, 0), {"tp": core})

    def mid_second(j):
        for o in range(seqs):
            mid_x[j, o].wait_recv()
        place = mids.at[j, side]
        mid_c[j, 1] = send(place, place, (mc_send, mc_recv), (j, 1), {"tp": core})

    def mid_third(j):
        for half in range(2):
            mid_c[j, half].wait_recv()
        heads_all = mids[j].reshape(tps * seqs * head, rows)
        for half, held in enumerate((t, side)):
            kept = xg[0, held, block_rows(j), :].astype(jnp.float32)
            place = xg.at[1, held, block_rows(j), :]
            place[...] = (kept + out_product(0, heads_all, held)).astype(jnp.bfloat16)
            new_c[j, half] = send(place, place, (nc_send, nc_recv), (j, half), {"tp": core})

    def mid_fourth(j):
        for half in range(2):
            new_c[j, half].wait_recv()
        project(1, j)

    mid_first(0)
    mid_first(1)
    relay_side(0, out_across, out_over)
    mid_second(0)
    mid_first(2)
    mid_second(1)
    mid_first(3)
    mid_second(2)
    qkv_ready = relay_qkv(1, qkv_fly)
    out_whole.wait_recv()
    for copy in out_over:
        copy.wait_recv()
    mid_third(0)
    mid_second(3)
    out_fly, out_whole = send_out(1)
    mid_third(1)
    for copy in qkv_ready:
        copy.wait_recv()
    mid_fourth(0)
    mid_third(2)
    mid_fourth(1)
    mid_third(3)
    mid_fourth(2)
    out_across, out_over = relay_out(1, out_fly)
    mid_fourth(3)

    for j in range(seqs):
        o_s[j] = attend_block(j)
    outgoing = [
        send(o_s.at[ahead(o)], ag.at[t, s], (az_send, az_recv), o, {"sp": ahead(o)}) for o in hops
    ]
    ag[t, s] = o_s[s]
    relay_side(1, out_across, out_over)
    for copy in outgoing:
        copy.wait_recv()
    block = ag.at[t]
    across = send(block, block, (at_send, at_recv), 0, {"tp": side})
    beside = send(block, block, (at_send, at_recv), 1, {"tp": core})
    out_whole.wait_recv()
    for copy in out_over:
        copy.wait_recv()
    across.wait_recv()
    block = ag.at[side]
    corner = send(block, block, (at_send, at_recv), 2, {"tp": core})
    beside.wait_recv()
    corner.wait_recv()
    heads_all = ag[...].reshape(tps * seqs * head, rows)
    last = []
    for half, held in enumerate((t, side)):
        kept = xg[1, held, block_rows(s), :].astype(jnp.float32)
        fin[held] = (kept + out_product(1, heads_all, held)).astype(jnp.bfloat16)
        place = fin.at[held]
        last.append(send(place, place, (fn_send, fn_recv), half, {"tp": core}))
    for copy in last:
        copy.wait_recv()
    for part in range(tps):
        out_ref[:, part * cols : (part + 1) * cols] = fin[part]
    for copy in started:
        copy.wait_send()
    for o in hops:
        for kind in range(3):
            tp_copy(kind, ahead(o)).wait_send()
    for way in (0, 1):
        for k in range(seqs - 1):
            copy, valid = onward(way, k)

            @pl.when(valid)
            def _(copy=copy):
                copy.wait_send()


def fused_device(
    sizes,
    stream,
    doc_ids,
    norm_gain,
    query_weight,
    key_weight,
    value_weight,
    out_weight,
    query_gain,
    key_gain,
    rel_bias,
):
    groups, seqs, tps = sizes
    rows, width = stream.shape
    cols = width // tps
    layers, deep, _ = query_weight.shape
    head = query_gain.shape[1]
    depth = -(-LEFT * SEG // rows)

    padded = jnp.pad(
        rel_bias, ((0, 0), (0, (depth + 2) * rows - rel_bias.shape[1])), mode="edge"
    )
    docs8 = jnp.broadcast_to(doc_ids.astype(jnp.float32)[None], (8, rows))
    dma = pltpu.SemaphoreType.DMA
    bf16 = jnp.bfloat16
    scratch = [
        pltpu.VMEM((layers, seqs, 3 * head, deep), bf16),
        pltpu.VMEM((layers, tps, seqs * rows, cols), bf16),
        pltpu.VMEM((layers, seqs, 3 * head, deep), bf16),
        pltpu.VMEM((layers, tps, seqs) + out_weight.shape[1:], bf16),
        pltpu.VMEM((seqs, 8, rows), jnp.float32),
        pltpu.VMEM((seqs, rows, 128), jnp.float32),
        pltpu.VMEM((seqs, tps, seqs, head, rows), bf16),
        pltpu.VMEM((tps, seqs, head, rows), bf16),
        pltpu.VMEM((tps, rows, cols), bf16),
        pltpu.VMEM((depth + 1, rows, rows), jnp.float32),
        pltpu.VMEM((rows, width), bf16),
        pltpu.VMEM((seqs, head, rows), bf16),
        pltpu.VMEM((seqs, rows, head), bf16),
        pltpu.VMEM((seqs, head, rows), bf16),
        pltpu.VMEM((seqs, head, rows), bf16),
    ]
    pairs = [
        (seqs,),
        (2, seqs),
        (3, seqs),
        (layers, seqs),
        (layers, seqs),
        (layers, seqs),
        (layers, seqs),
        (layers, seqs),
        (layers, seqs),
        (seqs, seqs),
        (seqs, seqs),
        (seqs, 2),
        (seqs, 2),
        (seqs,),
        (3,),
        (2,),
    ]
    scratch += [dma(shape) for shape in pairs for _ in range(2)]
    return pl.pallas_call(
        functools.partial(fused_kernel, sizes),
        name="fused_layers",
        out_shape=jax.ShapeDtypeStruct((rows, width), bf16),
        in_specs=[pl.BlockSpec(memory_space=pltpu.VMEM)] * 10,
        out_specs=pl.BlockSpec(memory_space=pltpu.VMEM),
        scratch_shapes=scratch,
        compiler_params=pltpu.CompilerParams(
            collective_id=0, has_side_effects=True, vmem_limit_bytes=60 * 1024 * 1024
        ),
    )(
        stream,
        docs8,
        norm_gain,
        query_weight,
        key_weight,
        value_weight,
        out_weight,
        query_gain,
        key_gain,
        padded,
    )


def solution(mesh):
    placed = (
        P(("grp", "sp"), None),
        P(("grp", "sp")),
        P(),
        P(None, "sp", "tp"),
        P(None, "sp", "tp"),
        P(None, "sp", "tp"),
        P(None, "sp", "tp"),
        P(),
        P(),
        P("tp", None),
    )
    sizes = tuple(mesh.shape[axis] for axis in ("grp", "sp", "tp"))

    def body(*args):
        one_head_each = args[-1].shape[0] == sizes[1]
        fits = sizes[0] == 2 and sizes[2] == 4 and args[0].shape[0] == MAXREL
        if one_head_each and fits:
            return fused_device(sizes, *args)
        return on_device(*args)

    return jax.shard_map(
        body, mesh=mesh, in_specs=placed, out_specs=P(("grp", "sp"), None), check_vma=False
    )
```

```python
import functools

import jax
import jax.numpy as jnp
from jax import lax
from jax.experimental import pallas as pl
from jax.experimental.pallas import tpu as pltpu
from jax.sharding import PartitionSpec as P

SEG = 64
LEFT = 8
MAXREL = 256
LAYERS = 2


epsilon = 1e-06


def shifted(value, axis, steps):
    count = lax.axis_size(axis)
    initial, last = (max(0, -steps), min(count, count - steps))
    return lax.ppermute(value, axis, [(source, source + steps) for source in range(initial, last)])


def row_norm(values, gain):
    return values * lax.rsqrt(jnp.mean(values * values, axis=-1, keepdims=True) + epsilon) * gain


def bias_table(rel_bias):
    heads_here = rel_bias.shape[0]
    reach = LEFT * SEG
    width = (LEFT + 1) * SEG
    highest = reach + SEG - 1
    reversed_bias = rel_bias[:, ::-1]
    upper_fill = jnp.broadcast_to(rel_bias[:, -1:], (heads_here, highest - MAXREL))
    flat_row = jnp.concatenate([upper_fill, reversed_bias[:, : MAXREL + SEG]], axis=1)
    lines = [
        flat_row[:, SEG - 1 - position : SEG - 1 - position + width] for position in range(SEG)
    ]
    return jnp.stack(lines, axis=1)


def attend(query, ext_keys, ext_values, ext_docs, own_docs, offset, table):
    rows, heads_here, head_size = query.shape
    count = rows // SEG
    width = (LEFT + 1) * SEG
    blocks = query.reshape(count, SEG, heads_here, head_size)
    key_blocks = ext_keys.reshape(count + LEFT, SEG, heads_here, head_size)
    value_blocks = ext_values.reshape(count + LEFT, SEG, heads_here, head_size)
    doc_blocks = ext_docs.reshape(count + LEFT, SEG)
    score_parts = [
        jnp.einsum(
            "nqhd,nkhd->nhqk",
            blocks,
            key_blocks[earlier : earlier + count],
            preferred_element_type=jnp.float32,
        )
        for earlier in range(LEFT + 1)
    ]
    scores = jnp.concatenate(score_parts, axis=-1)
    scores = scores * head_size ** (-0.5) + table[None]
    doc_band = jnp.concatenate(
        [doc_blocks[earlier : earlier + count] for earlier in range(LEFT + 1)], axis=1
    )
    key_pos = (
        offset
        + SEG * jnp.arange(count, dtype=jnp.int32)[:, None]
        - LEFT * SEG
        + jnp.arange(width, dtype=jnp.int32)[None, :]
    )
    allowed = (key_pos >= 0)[:, None, None, :] & (
        doc_band[:, None, None, :] == own_docs.reshape(count, SEG)[:, None, :, None]
    )
    scores = jnp.where(allowed, scores, -1e30)
    peak = jnp.max(scores, axis=-1, keepdims=True)
    expo = jnp.exp(scores - peak)
    weights = (expo / jnp.sum(expo, axis=-1, keepdims=True)).astype(jnp.bfloat16)
    mixed = jnp.zeros((count, SEG, heads_here, head_size), jnp.float32)
    for earlier in range(LEFT + 1):
        part_weights = weights[..., earlier * SEG : (earlier + 1) * SEG]
        mixed = mixed + jnp.einsum(
            "nhqk,nkhd->nqhd",
            part_weights,
            value_blocks[earlier : earlier + count],
            preferred_element_type=jnp.float32,
        )
    return mixed.astype(jnp.bfloat16).reshape(rows, heads_here * head_size)


def on_device(
    stream,
    doc_ids,
    norm_gain,
    query_weight,
    key_weight,
    value_weight,
    out_weight,
    query_gain,
    key_gain,
    rel_bias,
):
    rows = stream.shape[0]
    heads_here = rel_bias.shape[0]
    head_size = query_gain.shape[1]
    local_width = heads_here * head_size
    reach = LEFT * SEG
    depth = -(-reach // rows)
    offset = lax.axis_index("sp") * rows
    col_width = out_weight.shape[2]
    col_start = lax.axis_index("tp") * col_width
    table = bias_table(rel_bias)
    x = stream
    for layer in range(LAYERS):
        widened = x.astype(jnp.float32)
        normed = row_norm(widened, norm_gain[layer]).astype(jnp.bfloat16)
        own_cols = normed
        q_raw = jnp.dot(
            own_cols,
            lax.all_gather(query_weight[layer], "sp", axis=0, tiled=True),
            preferred_element_type=jnp.float32,
        )
        k_raw = jnp.dot(
            normed,
            lax.all_gather(key_weight[layer], "sp", axis=0, tiled=True),
            preferred_element_type=jnp.float32,
        )
        v_raw = jnp.dot(
            normed,
            lax.all_gather(value_weight[layer], "sp", axis=0, tiled=True),
            preferred_element_type=jnp.float32,
        )
        query = row_norm(q_raw.reshape(rows, heads_here, head_size), query_gain[layer]).astype(
            jnp.bfloat16
        )
        keys = row_norm(
            k_raw.reshape(normed.shape[0], heads_here, head_size), key_gain[layer]
        ).astype(jnp.bfloat16)
        values = v_raw.astype(jnp.bfloat16)
        flat_keys = keys.reshape(rows, local_width)
        tail = (flat_keys, values, doc_ids)
        received = [
            shifted((tail[0], tail[1], tail[2]), "sp", distance_back)
            for distance_back in range(depth, 0, -1)
        ]
        ext_keys = jnp.concatenate([item[0] for item in received] + [flat_keys], axis=0)
        ext_values = jnp.concatenate([item[1] for item in received] + [values], axis=0)
        ext_docs = jnp.concatenate([item[2] for item in received] + [doc_ids], axis=0)
        ext_keys = ext_keys.reshape(reach + rows, heads_here, head_size)
        ext_values = ext_values.reshape(reach + rows, heads_here, head_size)
        attended = attend(query, ext_keys, ext_values, ext_docs, doc_ids, offset, table)
        all_heads = lax.all_gather(attended, "tp", axis=1, tiled=True)
        projected = jnp.dot(
            all_heads,
            lax.all_gather(out_weight[layer], "sp", axis=0, tiled=True),
            preferred_element_type=jnp.float32,
        )
        own_cols = lax.dynamic_slice_in_dim(widened, col_start, col_width, 1)
        new_cols = (own_cols + projected).astype(jnp.bfloat16)
        x = lax.all_gather(new_cols, "tp", axis=1, tiled=True)
    return x


MESH = pl.DeviceIdType.MESH
NEG = -1e30


def fused_kernel(
    sizes,
    x_in,
    docs_ref,
    ngain_ref,
    qw_in,
    kw_in,
    vw_in,
    wo_in,
    qgain_ref,
    kgain_ref,
    bias_ref,
    out_ref,
    x_ref,
    qw_ref,
    kw_ref,
    vw_ref,
    woin_ref,
    load,
    wt_ref,
    xg,
    wq,
    wo,
    docs,
    dcol,
    mids,
    ag,
    fin,
    bias,
    nb,
    q_s,
    k_s,
    v_s,
    o_s,
    doc_send,
    doc_recv,
    xz_send,
    xz_recv,
    xt_send,
    xt_recv,
    wz_send,
    wz_recv,
    wy_send,
    wy_recv,
    oz_send,
    oz_recv,
    ox_send,
    ox_recv,
    oy_send,
    oy_recv,
    op_send,
    op_recv,
    mz_send,
    mz_recv,
    mx_send,
    mx_recv,
    mc_send,
    mc_recv,
    nc_send,
    nc_recv,
    rs_send,
    rs_recv,
    az_send,
    az_recv,
    at_send,
    at_recv,
    fn_send,
    fn_recv,
):
    groups, seqs, tps = sizes
    rows, width = x_ref.shape
    cols = width // tps
    head = qgain_ref.shape[1]
    layers = wt_ref.shape[0]
    depth = bias.shape[1] - 1
    parts = xz_send.shape[1]
    tall = rows // parts
    pair = bias.shape[0]
    grp = lax.axis_index("grp")
    s = lax.axis_index("sp")
    t = lax.axis_index("tp")
    other_grp = 1 - grp
    core = t + 1 - 2 * lax.rem(t, 2)
    side = lax.rem(t + 2, tps)
    inner = (s > 0) & (s < seqs - 1)
    near = jnp.clip(s, 1, seqs - 2)
    far = seqs - 1 - near
    first = jnp.where(inner, seqs - 1 - s, near)
    inside = near - 1
    edge = jnp.where(near == 1, 0, seqs - 1)
    beyond = seqs - 1 - edge
    started = []

    def remote(src, dst, sems, out_index, in_index, where):
        return pltpu.make_async_remote_copy(
            src_ref=src,
            dst_ref=dst,
            send_sem=sems[0].at[out_index],
            recv_sem=sems[1].at[in_index],
            device_id=where,
            device_id_type=MESH,
        )

    def send(src, dst, sems, index, where):
        copy = remote(src, dst, sems, index, index, where)
        copy.start()
        started.append(copy)
        return copy

    def settle():
        for copy in started:
            copy.wait_send()
        started.clear()

    def ahead(o):
        return lax.rem(s + o, seqs)

    def block_rows(i):
        return pl.ds(pl.multiple_of(i * rows, rows), rows)

    def cut_rows(i, h):
        return pl.ds(pl.multiple_of(i * rows + h * tall, tall), tall)

    loads = [
        pltpu.make_async_copy(src, dst, load.at[n])
        for n, (src, dst) in enumerate(
            zip((x_in, qw_in, kw_in, vw_in, wo_in), (x_ref, qw_ref, kw_ref, vw_ref, woin_ref))
        )
    ]
    for copy in loads:
        copy.start()
    barrier = pltpu.get_barrier_semaphore()
    partners = [{"sp": ahead(o)} for o in range(1, seqs)]
    partners += [{"tp": core}, {"tp": side}, {"grp": other_grp}]
    for where in partners:
        pl.semaphore_signal(barrier, inc=1, device_id=where, device_id_type=MESH)
    pl.semaphore_wait(barrier, len(partners))
    loads[0].wait()

    own_cols = pl.ds(pl.multiple_of(t * cols, cols), cols)
    ohalf = woin_ref.shape[1] // 2
    opart = pl.ds(pl.multiple_of(grp * ohalf, ohalf), ohalf)
    hops = list(range(1, seqs))

    def x_copy(source, dest, h):
        place = xg.at[0, t, cut_rows(source, h), :]
        return remote(
            x_ref.at[h * tall : (h + 1) * tall, own_cols],
            place,
            (xz_send, xz_recv),
            (dest, h),
            (source, h),
            {"sp": dest},
        )

    def w_copy(layer, source, dest):
        return remote(
            wt_ref.at[layer, pair * (dest - 1) + grp],
            wq.at[layer, source, grp],
            (wz_send, wz_recv),
            (layer, dest),
            (layer, source),
            {"sp": dest},
        )

    def o_copy(layer, source, dest):
        return remote(
            woin_ref.at[layer, opart, :],
            wo.at[layer, t, source, opart, :],
            (oz_send, oz_recv),
            (layer, dest),
            (layer, source),
            {"sp": dest},
        )

    def w_near(layer, source):
        return remote(
            wt_ref.at[layer, pl.ds(pair * inside, pair)],
            wq.at[layer, source],
            (wz_send, wz_recv),
            (layer, near),
            (layer, source),
            {"sp": near},
        )

    def o_near(layer, source):
        return remote(
            woin_ref.at[layer],
            wo.at[layer, t, source],
            (oz_send, oz_recv),
            (layer, near),
            (layer, source),
            {"sp": near},
        )

    def outer_plan(n):
        if n == 0:
            return [x_copy(s, near, h) for h in range(parts)]
        if n == 1:
            x_far = [x_copy(s, far, h) for h in range(parts)]
            return [w_copy(0, s, near), x_far[0], w_copy(0, s, far)] + x_far[1:]
        if n == 2:
            return [o_copy(0, s, far), o_near(0, s)]
        plan = [w_copy(1, s, far), w_copy(1, s, near)]
        return plan + [o_copy(1, s, far), o_near(1, s), o_copy(1, s, seqs - 1 - s)]

    def inner_plan(n):
        other = seqs - 1 - s
        if n == 0:
            return [x_copy(s, other, h) for h in range(parts)]
        if n == 1:
            return [w_copy(0, s, other)]
        if n == 2:
            return [o_copy(0, s, other), w_copy(1, s, other)]
        return [o_copy(1, s, ahead(o)) for o in hops]

    def sends(plan, n, act):
        for copy in plan(n):
            getattr(copy, act)()

    def tp_copy(kind, block, h):
        held = side if kind == 2 else t
        place = xg.at[0, held, cut_rows(block, h), :]
        index = (kind, block, h)
        where = {"tp": side if kind == 1 else core}
        return remote(place, place, (xt_send, xt_recv), index, index, where)

    def w_relay(layer, block):
        place = wq.at[layer, block, grp]
        index = (layer, block)
        return remote(place, place, (wy_send, wy_recv), index, index, {"grp": other_grp})

    def o_relay(layer, kind, block):
        held = side if kind == 2 else t
        place = wo.at[layer, held, block, opart, :]
        sems = ((ox_send, ox_recv), (oy_send, oy_recv), (op_send, op_recv))[kind]
        index = (layer, block)
        where = {"tp": side} if kind == 0 else {"grp": other_grp}
        return remote(place, place, sems, index, index, where)

    def o_whole(layer):
        place = wo.at[layer, t, s]
        index = (layer, s)
        return remote(woin_ref.at[layer], place, (ox_send, ox_recv), index, index, {"tp": side})

    def begin(copy):
        copy.start()
        started.append(copy)

    def fan(block, h):
        x_copy(block, near, h).wait_recv()
        begin(tp_copy(1, block, h))
        begin(tp_copy(0, block, h))

    def pass_on(block, h):
        tp_copy(1, block, h).wait_recv()
        begin(tp_copy(2, block, h))

    def spread_w(layer, block):
        w_copy(layer, block, near).wait_recv()
        begin(w_relay(layer, block))

    def spread_o(layer, block, whole=False):
        (o_near(layer, block) if whole else o_copy(layer, block, near)).wait_recv()
        begin(o_relay(layer, 0, block))
        if not whole:
            begin(o_relay(layer, 1, block))

    def side_o(layer, block):
        o_relay(layer, 0, block).wait_recv()
        begin(o_relay(layer, 2, block))

    def ready_o(layer, relayed, sides):
        o_whole(layer).wait_recv()
        for block in relayed:
            o_relay(layer, 1, block).wait_recv()
        for block in sides:
            o_relay(layer, 2, block).wait_recv()

    def turn(layer):
        for which, source in enumerate((qw_ref, kw_ref, vw_ref)):
            turned = jnp.transpose(source[layer])
            for i in range(seqs):
                wt_ref[layer, i, which * head : (which + 1) * head, :] = turned[
                    i * head : (i + 1) * head, :
                ]

    @pl.when(inner)
    def _():
        sends(inner_plan, 0, "start")

    @pl.when(jnp.logical_not(inner))
    def _():
        sends(outer_plan, 0, "start")

    docs[s] = jnp.broadcast_to(docs_ref[...].astype(jnp.float32), docs.shape[1:])
    doc_c = [
        remote(docs.at[s], docs.at[s], (doc_send, doc_recv), o, o, {"sp": ahead(o)}) for o in hops
    ]
    for copy in doc_c:
        copy.start()
    for copy in loads[1:]:
        copy.wait()
    turn(0)

    @pl.when(inner)
    def _():
        sends(inner_plan, 1, "start")

    @pl.when(jnp.logical_not(inner))
    def _():
        for n in (1, 2):
            sends(outer_plan, n, "start")

    for layer in range(1, layers):
        turn(layer)

    @pl.when(jnp.logical_not(inner))
    def _():
        sends(outer_plan, 3, "start")

    for layer in range(layers):
        wo[layer, t, s] = woin_ref[layer]
    assert not started

    def project(layer, i):
        total = jnp.zeros((rows, 1), jnp.float32)
        for part in range(tps):
            piece = xg[layer, part, block_rows(i), :].astype(jnp.float32)
            total = total + jnp.sum(piece * piece, axis=1, keepdims=True)
        factor = lax.rsqrt(total * (1.0 / width) + epsilon)
        for part in range(tps):
            piece = xg[layer, part, block_rows(i), :].astype(jnp.float32)
            gain = ngain_ref[layer : layer + 1, part * cols : (part + 1) * cols]
            nb[:, part * cols : (part + 1) * cols] = (piece * factor * gain).astype(jnp.bfloat16)
        span = width // seqs
        raw = jnp.zeros((pair * 3 * head, rows), jnp.float32)
        for part in range(seqs):
            raw = raw + lax.dot_general(
                wq[layer, part].reshape(pair * 3 * head, span),
                nb[:, part * span : (part + 1) * span],
                (((1,), (1,)), ((), ())),
                preferred_element_type=jnp.float32,
            )

        def normal(value, gain):
            mean = jnp.mean(value * value, axis=0, keepdims=True)
            column = jnp.transpose(jnp.broadcast_to(gain, (128, head)))[:, 0:1]
            return value * lax.rsqrt(mean + epsilon) * column

        for a in range(pair):
            query, keys, values = [
                raw[(3 * a + n) * head : (3 * a + n + 1) * head] for n in range(3)
            ]
            query = normal(query, qgain_ref[layer : layer + 1, :]) * head ** (-0.5)
            keys = normal(keys, kgain_ref[layer : layer + 1, :])
            q_s[a, i] = query.astype(jnp.bfloat16)
            k_s[a, i] = jnp.transpose(keys).astype(jnp.bfloat16)
            v_s[a, i] = values.astype(jnp.bfloat16)

    def attend_block(j, a):
        pieces = []
        for i in range(max(0, j - depth), j + 1):
            score = jnp.dot(k_s[a, i], q_s[a, j], preferred_element_type=jnp.float32)
            same = dcol[i][:, 0:1] == docs[j, 0:1, :]
            pieces.append((i, jnp.where(same, score + bias[a, j - i], NEG)))
        peak = pieces[0][1].max(axis=0, keepdims=True)
        for _, piece in pieces[1:]:
            peak = jnp.maximum(peak, piece.max(axis=0, keepdims=True))
        mass = jnp.zeros((1, rows), jnp.float32)
        mixed = jnp.zeros((head, rows), jnp.float32)
        for i, piece in pieces:
            expo = jnp.exp(piece - peak)
            mass = mass + jnp.sum(expo, axis=0, keepdims=True)
            mixed = mixed + jnp.dot(
                v_s[a, i], expo.astype(jnp.bfloat16), preferred_element_type=jnp.float32
            )
        return (mixed / mass).astype(jnp.bfloat16)

    def out_product(layer, heads_all, held):
        return lax.dot_general(
            heads_all,
            wo[layer, held].reshape(-1, cols),
            (((0,), (0,)), ((), ())),
            preferred_element_type=jnp.float32,
        )

    def rest_copy(half, held):
        place = xg.at[1, held, block_rows(edge), :]
        return remote(place, place, (rs_send, rs_recv), half, half, {"sp": edge})

    def last_copy(j):
        return remote(
            o_s.at[j], ag.at[t, inside], (az_send, az_recv), j, inside, {"sp": j}
        )

    @pl.when(inner)
    def _():
        other = seqs - 1 - s
        for part in range(tps):
            xg[0, part, block_rows(s), :] = x_ref[:, part * cols : (part + 1) * cols]
        for layer in range(layers):
            wq[layer, s] = wt_ref[layer, pl.ds(pair * inside, pair)]
        begin(o_whole(0))
        key_seg = lax.broadcasted_iota(jnp.int32, (rows, rows), 0) // SEG
        query_seg = lax.broadcasted_iota(jnp.int32, (rows, rows), 1) // SEG
        entries = (bias_ref.shape[1] - 1) // 128 * 128
        tables = []
        for a in range(pair):
            line = bias_ref[pl.ds(pair * inside + a, 1), :]
            line, final = line[:, :entries], line[:, entries:]
            tables.append(
                jnp.concatenate(
                    [line, jnp.broadcast_to(final, (1, (depth + 2) * rows - entries))], axis=1
                )
            )
        for d in range(depth + 1):
            gap = query_seg + (d * rows) // SEG - key_seg
            for a in range(pair):
                spread = jnp.broadcast_to(
                    tables[a][:, d * rows : (d + 2) * rows], (rows, 2 * rows)
                )
                rolled = pltpu.roll(spread, 0, 1, stride=1, stride_axis=0)
                bias[a, d] = jnp.where((gap >= 0) & (gap <= LEFT), rolled[:, rows:], NEG)
        order = [(block, h) for h in range(parts) for block in (edge, other)]
        fan(*order[0])
        fan(*order[1])
        for copy in doc_c:
            copy.wait_recv()
        for i in range(seqs):
            dcol[i] = jnp.transpose(jnp.broadcast_to(docs[i, 0:1, :], (128, rows)))
        pass_on(*order[0])
        fan(*order[2])
        fan(*order[3])
        pass_on(*order[1])
        spread_w(0, edge)
        spread_w(0, other)
        pass_on(*order[2])
        fan(beyond, 0)
        pass_on(*order[3])
        spread_w(0, beyond)
        sends(inner_plan, 2, "start")
        for h in range(1, parts):
            fan(beyond, h)
        pass_on(beyond, 0)
        for h in range(1, parts):
            pass_on(beyond, h)
        for block in (edge, other, beyond):
            w_relay(0, block).wait_recv()
        project(0, s)
        spread_o(0, other)
        for block in (edge, other, beyond):
            for h in range(parts):
                tp_copy(0, block, h).wait_recv()
                tp_copy(2, block, h).wait_recv()
            project(0, block)
            if block is edge:
                spread_o(0, edge, True)
            if block is other:
                spread_o(0, beyond)

        mid_z, mid_x, mid_c, new_c = {}, {}, {}, {}
        turns = (0, 3, 1, 2)
        for n, j in enumerate(turns):
            for a in range(pair):
                mids[j, t, inside, a * head : (a + 1) * head, :] = attend_block(j, a)
            place = mids.at[j, t, inside]
            mid_z[j] = send(place, place, (mz_send, mz_recv), j, {"sp": other})
            mid_x[j, 0] = send(place, place, (mx_send, mx_recv), (j, 0), {"tp": side})
            if n == 0:
                side_o(0, other)
            if n == 1:
                side_o(0, edge)
            if n == 2:
                spread_w(1, other)

        def mid_first(j):
            mid_z[j].wait_recv()
            place = mids.at[j, t, 1 - inside]
            mid_x[j, 1] = send(place, place, (mx_send, mx_recv), (j, 1), {"tp": side})
            place = mids.at[j, t]
            mid_c[j, 0] = send(place, place, (mc_send, mc_recv), (j, 0), {"tp": core})

        def mid_second(j):
            for n in range(2):
                mid_x[j, n].wait_recv()
            place = mids.at[j, side]
            mid_c[j, 1] = send(place, place, (mc_send, mc_recv), (j, 1), {"tp": core})

        def mid_third(j):
            for half in range(2):
                mid_c[j, half].wait_recv()
            heads_all = mids[j].reshape(tps * seqs * head, rows)
            for half, held in enumerate((t, side)):
                kept = xg[0, held, block_rows(j), :].astype(jnp.float32)
                place = xg.at[1, held, block_rows(j), :]
                place[...] = (kept + out_product(0, heads_all, held)).astype(jnp.bfloat16)
                new_c[j, half] = send(place, place, (nc_send, nc_recv), (j, half), {"tp": core})
                if j in (0, seqs - 1):

                    @pl.when(edge == j)
                    def _(half=half, held=held):
                        rest_copy(half, held).start()

        def mid_fourth(j):
            for half in range(2):
                new_c[j, half].wait_recv()
            project(1, j)

        mid_first(0)
        side_o(0, beyond)
        mid_first(3)
        mid_second(0)
        spread_w(1, beyond)
        mid_first(1)
        mid_second(3)
        mid_first(2)
        mid_second(1)
        mid_second(2)
        spread_w(1, edge)
        begin(o_whole(1))
        sends(inner_plan, 3, "start")
        ready_o(0, (other, beyond), (edge, other, beyond))
        mid_third(0)
        mid_third(3)
        spread_o(1, beyond)
        mid_third(1)
        w_relay(1, edge).wait_recv()
        for block in (other, beyond):
            w_relay(1, block).wait_recv()
        mid_fourth(0)
        spread_o(1, other)
        mid_third(2)
        mid_fourth(3)
        spread_o(1, edge, True)
        side_o(1, beyond)
        mid_fourth(1)
        side_o(1, other)
        mid_fourth(2)
        for n, j in enumerate((0, seqs - 1, 1, 2)):
            for a in range(pair):
                o_s[j, a * head : (a + 1) * head, :] = attend_block(j, a)

            @pl.when(s != j)
            def _(j=j):
                last_copy(j).start()

            if n == 0:
                side_o(1, edge)
        ag[t, inside] = o_s[s]
        ag_in = remote(o_s.at[0], ag.at[t, 1 - inside], (az_send, az_recv), s, 1 - inside, {"sp": other})
        ag_in.wait_recv()
        ready_o(1, (other, beyond), (edge, other, beyond))
        for half, held in enumerate((t, side)):
            rest_copy(half, held).wait_send()
        for o in hops:
            last_copy(ahead(o)).wait_send()
        for n in range(4):
            sends(inner_plan, n, "wait_send")
        settle()

    @pl.when(jnp.logical_not(inner))
    def _():
        begin(o_whole(1))
        for copy in doc_c:
            copy.wait_recv()
        for block in (near, far, seqs - 1 - s):
            spread_o(1, block)
        for o in hops:
            side_o(1, ahead(o))
        for half, held in enumerate((t, side)):
            rest_copy(half, held).wait_recv()
        for n in range(2):
            place = ag.at[t, n]
            remote(place, place, (az_send, az_recv), s, n, {"sp": near}).wait_recv()
        ready_o(1, [ahead(o) for o in hops], [ahead(o) for o in hops])
        settle()
        for n in range(4):
            sends(outer_plan, n, "wait_send")

    block = ag.at[t]
    across = send(block, block, (at_send, at_recv), 0, {"tp": side})
    beside = send(block, block, (at_send, at_recv), 1, {"tp": core})
    across.wait_recv()
    block = ag.at[side]
    corner = send(block, block, (at_send, at_recv), 2, {"tp": core})
    beside.wait_recv()
    corner.wait_recv()
    heads_all = ag[...].reshape(tps * seqs * head, rows)
    last = []
    for half, held in enumerate((t, side)):
        kept = xg[1, held, block_rows(s), :].astype(jnp.float32)
        fin[held] = (kept + out_product(1, heads_all, held)).astype(jnp.bfloat16)
        place = fin.at[held]
        last.append(send(place, place, (fn_send, fn_recv), half, {"tp": core}))
    for copy in last:
        copy.wait_recv()
    for part in range(tps):
        out_ref[:, part * cols : (part + 1) * cols] = fin[part]
    settle()
    for copy in doc_c:
        copy.wait_send()

def fused_device(
    sizes,
    stream,
    doc_ids,
    norm_gain,
    query_weight,
    key_weight,
    value_weight,
    out_weight,
    query_gain,
    key_gain,
    rel_bias,
):
    groups, seqs, tps = sizes
    rows, width = stream.shape
    cols = width // tps
    layers, deep, _ = query_weight.shape
    head = query_gain.shape[1]
    depth = -(-LEFT * SEG // rows)

    dma = pltpu.SemaphoreType.DMA
    bf16 = jnp.bfloat16
    pair = seqs // 2
    whole = [stream, query_weight, key_weight, value_weight, out_weight]
    scratch = [pltpu.VMEM(one.shape, one.dtype) for one in whole] + [dma((len(whole),))]
    scratch += [
        pltpu.VMEM((layers, seqs, 3 * head, deep), bf16),
        pltpu.VMEM((layers, tps, seqs * rows, cols), bf16),
        pltpu.VMEM((layers, seqs, pair, 3 * head, deep), bf16),
        pltpu.VMEM((layers, tps, seqs) + out_weight.shape[1:], bf16),
        pltpu.VMEM((seqs, 8, rows), jnp.float32),
        pltpu.VMEM((seqs, rows, 128), jnp.float32),
        pltpu.VMEM((seqs, tps, 2, pair * head, rows), bf16),
        pltpu.VMEM((tps, 2, pair * head, rows), bf16),
        pltpu.VMEM((tps, rows, cols), bf16),
        pltpu.VMEM((pair, depth + 1, rows, rows), jnp.float32),
        pltpu.VMEM((rows, width), bf16),
        pltpu.VMEM((pair, seqs, head, rows), bf16),
        pltpu.VMEM((pair, seqs, rows, head), bf16),
        pltpu.VMEM((pair, seqs, head, rows), bf16),
        pltpu.VMEM((seqs, pair * head, rows), bf16),
    ]
    pairs = [
        (seqs,),
        (seqs, 2),
        (3, seqs, 2),
        (layers, seqs),
        (layers, seqs),
        (layers, seqs),
        (layers, seqs),
        (layers, seqs),
        (layers, seqs),
        (seqs,),
        (seqs, 2),
        (seqs, 2),
        (seqs, 2),
        (2,),
        (seqs,),
        (3,),
        (2,),
    ]
    scratch += [dma(shape) for shape in pairs for _ in range(2)]
    return pl.pallas_call(
        functools.partial(fused_kernel, sizes),
        name="fused_layers",
        out_shape=jax.ShapeDtypeStruct((rows, width), bf16),
        in_specs=[
            pl.BlockSpec(memory_space=pltpu.HBM if n in (0, 3, 4, 5, 6) else pltpu.VMEM)
            for n in range(10)
        ],
        out_specs=pl.BlockSpec(memory_space=pltpu.VMEM),
        scratch_shapes=scratch,
        compiler_params=pltpu.CompilerParams(
            collective_id=0, has_side_effects=True, vmem_limit_bytes=58 * 1024 * 1024
        ),
    )(
        stream,
        doc_ids[None],
        norm_gain,
        query_weight,
        key_weight,
        value_weight,
        out_weight,
        query_gain,
        key_gain,
        rel_bias,
    )


def solution(mesh):
    placed = (
        P(("grp", "sp"), None),
        P(("grp", "sp")),
        P(),
        P(None, "sp", "tp"),
        P(None, "sp", "tp"),
        P(None, "sp", "tp"),
        P(None, "sp", "tp"),
        P(),
        P(),
        P("tp", None),
    )
    sizes = tuple(mesh.shape[axis] for axis in ("grp", "sp", "tp"))

    def body(*args):
        one_head_each = args[-1].shape[0] == sizes[1]
        fits = sizes == (2, 4, 4) and args[0].shape[0] == MAXREL
        if one_head_each and fits:
            return fused_device(sizes, *args)
        return on_device(*args)

    return jax.shard_map(
        body, mesh=mesh, in_specs=placed, out_specs=P(("grp", "sp"), None), check_vma=False
    )
```

```python
import functools

import jax
import jax.numpy as jnp
from jax import lax
from jax.experimental import pallas as pl
from jax.experimental.pallas import tpu as pltpu
from jax.sharding import PartitionSpec as P

SEG = 64
LEFT = 8
MAXREL = 256
LAYERS = 2


epsilon = 1e-06


def shifted(value, axis, steps):
    count = lax.axis_size(axis)
    initial, last = (max(0, -steps), min(count, count - steps))
    return lax.ppermute(value, axis, [(source, source + steps) for source in range(initial, last)])


def row_norm(values, gain):
    return values * lax.rsqrt(jnp.mean(values * values, axis=-1, keepdims=True) + epsilon) * gain


def bias_table(rel_bias):
    heads_here = rel_bias.shape[0]
    reach = LEFT * SEG
    width = (LEFT + 1) * SEG
    highest = reach + SEG - 1
    reversed_bias = rel_bias[:, ::-1]
    upper_fill = jnp.broadcast_to(rel_bias[:, -1:], (heads_here, highest - MAXREL))
    flat_row = jnp.concatenate([upper_fill, reversed_bias[:, : MAXREL + SEG]], axis=1)
    lines = [
        flat_row[:, SEG - 1 - position : SEG - 1 - position + width] for position in range(SEG)
    ]
    return jnp.stack(lines, axis=1)


def attend(query, ext_keys, ext_values, ext_docs, own_docs, offset, table):
    rows, heads_here, head_size = query.shape
    count = rows // SEG
    width = (LEFT + 1) * SEG
    blocks = query.reshape(count, SEG, heads_here, head_size)
    key_blocks = ext_keys.reshape(count + LEFT, SEG, heads_here, head_size)
    value_blocks = ext_values.reshape(count + LEFT, SEG, heads_here, head_size)
    doc_blocks = ext_docs.reshape(count + LEFT, SEG)
    score_parts = [
        jnp.einsum(
            "nqhd,nkhd->nhqk",
            blocks,
            key_blocks[earlier : earlier + count],
            preferred_element_type=jnp.float32,
        )
        for earlier in range(LEFT + 1)
    ]
    scores = jnp.concatenate(score_parts, axis=-1)
    scores = scores * head_size ** (-0.5) + table[None]
    doc_band = jnp.concatenate(
        [doc_blocks[earlier : earlier + count] for earlier in range(LEFT + 1)], axis=1
    )
    key_pos = (
        offset
        + SEG * jnp.arange(count, dtype=jnp.int32)[:, None]
        - LEFT * SEG
        + jnp.arange(width, dtype=jnp.int32)[None, :]
    )
    allowed = (key_pos >= 0)[:, None, None, :] & (
        doc_band[:, None, None, :] == own_docs.reshape(count, SEG)[:, None, :, None]
    )
    scores = jnp.where(allowed, scores, -1e30)
    peak = jnp.max(scores, axis=-1, keepdims=True)
    expo = jnp.exp(scores - peak)
    weights = (expo / jnp.sum(expo, axis=-1, keepdims=True)).astype(jnp.bfloat16)
    mixed = jnp.zeros((count, SEG, heads_here, head_size), jnp.float32)
    for earlier in range(LEFT + 1):
        part_weights = weights[..., earlier * SEG : (earlier + 1) * SEG]
        mixed = mixed + jnp.einsum(
            "nhqk,nkhd->nqhd",
            part_weights,
            value_blocks[earlier : earlier + count],
            preferred_element_type=jnp.float32,
        )
    return mixed.astype(jnp.bfloat16).reshape(rows, heads_here * head_size)


def on_device(
    stream,
    doc_ids,
    norm_gain,
    query_weight,
    key_weight,
    value_weight,
    out_weight,
    query_gain,
    key_gain,
    rel_bias,
):
    rows = stream.shape[0]
    heads_here = rel_bias.shape[0]
    head_size = query_gain.shape[1]
    local_width = heads_here * head_size
    reach = LEFT * SEG
    depth = -(-reach // rows)
    offset = lax.axis_index("sp") * rows
    col_width = out_weight.shape[2]
    col_start = lax.axis_index("tp") * col_width
    table = bias_table(rel_bias)
    x = stream
    for layer in range(LAYERS):
        widened = x.astype(jnp.float32)
        normed = row_norm(widened, norm_gain[layer]).astype(jnp.bfloat16)
        own_cols = normed
        q_raw = jnp.dot(
            own_cols,
            lax.all_gather(query_weight[layer], "sp", axis=0, tiled=True),
            preferred_element_type=jnp.float32,
        )
        k_raw = jnp.dot(
            normed,
            lax.all_gather(key_weight[layer], "sp", axis=0, tiled=True),
            preferred_element_type=jnp.float32,
        )
        v_raw = jnp.dot(
            normed,
            lax.all_gather(value_weight[layer], "sp", axis=0, tiled=True),
            preferred_element_type=jnp.float32,
        )
        query = row_norm(q_raw.reshape(rows, heads_here, head_size), query_gain[layer]).astype(
            jnp.bfloat16
        )
        keys = row_norm(
            k_raw.reshape(normed.shape[0], heads_here, head_size), key_gain[layer]
        ).astype(jnp.bfloat16)
        values = v_raw.astype(jnp.bfloat16)
        flat_keys = keys.reshape(rows, local_width)
        tail = (flat_keys, values, doc_ids)
        received = [
            shifted((tail[0], tail[1], tail[2]), "sp", distance_back)
            for distance_back in range(depth, 0, -1)
        ]
        ext_keys = jnp.concatenate([item[0] for item in received] + [flat_keys], axis=0)
        ext_values = jnp.concatenate([item[1] for item in received] + [values], axis=0)
        ext_docs = jnp.concatenate([item[2] for item in received] + [doc_ids], axis=0)
        ext_keys = ext_keys.reshape(reach + rows, heads_here, head_size)
        ext_values = ext_values.reshape(reach + rows, heads_here, head_size)
        attended = attend(query, ext_keys, ext_values, ext_docs, doc_ids, offset, table)
        all_heads = lax.all_gather(attended, "tp", axis=1, tiled=True)
        projected = jnp.dot(
            all_heads,
            lax.all_gather(out_weight[layer], "sp", axis=0, tiled=True),
            preferred_element_type=jnp.float32,
        )
        own_cols = lax.dynamic_slice_in_dim(widened, col_start, col_width, 1)
        new_cols = (own_cols + projected).astype(jnp.bfloat16)
        x = lax.all_gather(new_cols, "tp", axis=1, tiled=True)
    return x


MESH = pl.DeviceIdType.MESH
NEG = -1e30


def fused_kernel(
    sizes,
    x_in,
    docs_ref,
    ngain_ref,
    qw_in,
    kw_in,
    vw_in,
    wo_in,
    qgain_ref,
    kgain_ref,
    bias_ref,
    out_ref,
    x_ref,
    qw_ref,
    kw_ref,
    vw_ref,
    woin_ref,
    load,
    wt_ref,
    xg,
    wq,
    wo,
    docs,
    dcol,
    mids,
    ag,
    fin,
    bias,
    nb,
    q_s,
    k_s,
    v_s,
    o_s,
    doc_send,
    doc_recv,
    xz_send,
    xz_recv,
    xt_send,
    xt_recv,
    wz_send,
    wz_recv,
    wy_send,
    wy_recv,
    oz_send,
    oz_recv,
    ox_send,
    ox_recv,
    oy_send,
    oy_recv,
    op_send,
    op_recv,
    mz_send,
    mz_recv,
    mx_send,
    mx_recv,
    mc_send,
    mc_recv,
    nc_send,
    nc_recv,
    rs_send,
    rs_recv,
    az_send,
    az_recv,
    at_send,
    at_recv,
    fn_send,
    fn_recv,
):
    groups, seqs, tps = sizes
    rows, width = x_ref.shape
    cols = width // tps
    head = qgain_ref.shape[1]
    layers = wt_ref.shape[0]
    depth = bias.shape[1] - 1
    parts = xz_send.shape[1]
    tall = rows // parts
    pair = bias.shape[0]
    grp = lax.axis_index("grp")
    s = lax.axis_index("sp")
    t = lax.axis_index("tp")
    other_grp = 1 - grp
    core = t + 1 - 2 * lax.rem(t, 2)
    side = lax.rem(t + 2, tps)
    inner = (s > 0) & (s < seqs - 1)
    near = jnp.clip(s, 1, seqs - 2)
    far = seqs - 1 - near
    first = jnp.where(inner, seqs - 1 - s, near)
    inside = near - 1
    edge = jnp.where(near == 1, 0, seqs - 1)
    beyond = seqs - 1 - edge
    started = []

    def remote(src, dst, sems, out_index, in_index, where):
        return pltpu.make_async_remote_copy(
            src_ref=src,
            dst_ref=dst,
            send_sem=sems[0].at[out_index],
            recv_sem=sems[1].at[in_index],
            device_id=where,
            device_id_type=MESH,
        )

    def send(src, dst, sems, index, where):
        copy = remote(src, dst, sems, index, index, where)
        copy.start()
        started.append(copy)
        return copy

    def settle():
        for copy in started:
            copy.wait_send()
        started.clear()

    def ahead(o):
        return lax.rem(s + o, seqs)

    def block_rows(i):
        return pl.ds(pl.multiple_of(i * rows, rows), rows)

    def cut_rows(i, h):
        return pl.ds(pl.multiple_of(i * rows + h * tall, tall), tall)

    loads = [
        pltpu.make_async_copy(src, dst, load.at[n])
        for n, (src, dst) in enumerate(
            zip((x_in, qw_in, kw_in, vw_in, wo_in), (x_ref, qw_ref, kw_ref, vw_ref, woin_ref))
        )
    ]
    for copy in loads:
        copy.start()
    barrier = pltpu.get_barrier_semaphore()
    partners = [{"sp": ahead(o)} for o in range(1, seqs)]
    partners += [{"tp": core}, {"tp": side}, {"grp": other_grp}]
    for where in partners:
        pl.semaphore_signal(barrier, inc=1, device_id=where, device_id_type=MESH)
    pl.semaphore_wait(barrier, len(partners))
    loads[0].wait()

    own_cols = pl.ds(pl.multiple_of(t * cols, cols), cols)
    ohalf = woin_ref.shape[1] // 2
    opart = pl.ds(pl.multiple_of(grp * ohalf, ohalf), ohalf)
    hops = list(range(1, seqs))

    def x_copy(source, dest, h):
        place = xg.at[0, t, cut_rows(source, h), :]
        return remote(
            x_ref.at[h * tall : (h + 1) * tall, own_cols],
            place,
            (xz_send, xz_recv),
            (dest, h),
            (source, h),
            {"sp": dest},
        )

    def w_copy(layer, source, dest):
        return remote(
            wt_ref.at[layer, pair * (dest - 1) + grp],
            wq.at[layer, source, grp],
            (wz_send, wz_recv),
            (layer, dest),
            (layer, source),
            {"sp": dest},
        )

    def o_copy(layer, source, dest):
        return remote(
            woin_ref.at[layer, opart, :],
            wo.at[layer, t, source, opart, :],
            (oz_send, oz_recv),
            (layer, dest),
            (layer, source),
            {"sp": dest},
        )

    def w_full(layer, source, dest):
        return remote(
            wt_ref.at[layer, pl.ds(pair * (dest - 1), pair)],
            wq.at[layer, source],
            (wz_send, wz_recv),
            (layer, dest),
            (layer, source),
            {"sp": dest},
        )

    def o_full(layer, source, dest):
        return remote(
            woin_ref.at[layer],
            wo.at[layer, t, source],
            (oz_send, oz_recv),
            (layer, dest),
            (layer, source),
            {"sp": dest},
        )

    def outer_plan(n):
        if n == 0:
            return [x_copy(s, near, h) for h in range(parts)]
        if n == 1:
            x_far = [x_copy(s, far, h) for h in range(parts)]
            return [w_copy(0, s, near)] + x_far + [w_copy(0, s, far)]
        if n == 2:
            return [o_copy(0, s, far), o_full(0, s, near)]
        plan = [w_copy(1, s, near), w_copy(1, s, far)]
        return plan + [o_copy(1, s, far), o_full(1, s, near), o_copy(1, s, seqs - 1 - s)]

    def inner_plan(n):
        other = seqs - 1 - s
        if n == 0:
            return [x_copy(s, other, h) for h in range(parts)]
        if n == 1:
            return [w_copy(0, s, other), o_full(1, s, edge)]
        if n == 2:
            return [o_copy(0, s, other), w_copy(1, s, other)]
        return [o_copy(1, s, other), o_copy(1, s, beyond)]

    def sends(plan, n, act):
        for copy in plan(n):
            getattr(copy, act)()

    def tp_copy(kind, block, h):
        held = side if kind == 2 else t
        place = xg.at[0, held, cut_rows(block, h), :]
        index = (kind, block, h)
        where = {"tp": side if kind == 1 else core}
        return remote(place, place, (xt_send, xt_recv), index, index, where)

    def w_relay(layer, block):
        place = wq.at[layer, block, grp]
        index = (layer, block)
        return remote(place, place, (wy_send, wy_recv), index, index, {"grp": other_grp})

    def o_relay(layer, kind, block):
        held = side if kind == 2 else t
        place = wo.at[layer, held, block, opart, :]
        sems = ((ox_send, ox_recv), (oy_send, oy_recv), (op_send, op_recv))[kind]
        index = (layer, block)
        where = {"tp": side} if kind == 0 else {"grp": other_grp}
        return remote(place, place, sems, index, index, where)

    def o_whole(layer):
        place = wo.at[layer, t, s]
        index = (layer, s)
        return remote(woin_ref.at[layer], place, (ox_send, ox_recv), index, index, {"tp": side})

    def begin(copy):
        copy.start()
        started.append(copy)

    def fan(block, h):
        x_copy(block, near, h).wait_recv()
        begin(tp_copy(1, block, h))
        begin(tp_copy(0, block, h))

    def pass_on(block, h):
        tp_copy(1, block, h).wait_recv()
        begin(tp_copy(2, block, h))

    def spread_w(layer, block):
        w_copy(layer, block, near).wait_recv()
        begin(w_relay(layer, block))

    def spread_o(layer, block, whole=False):
        (o_full(layer, block, near) if whole else o_copy(layer, block, near)).wait_recv()
        begin(o_relay(layer, 0, block))
        if not whole:
            begin(o_relay(layer, 1, block))

    def side_o(layer, block):
        o_relay(layer, 0, block).wait_recv()
        begin(o_relay(layer, 2, block))

    def ready_o(layer, relayed, sides):
        o_whole(layer).wait_recv()
        for block in relayed:
            o_relay(layer, 1, block).wait_recv()
        for block in sides:
            o_relay(layer, 2, block).wait_recv()

    def turn(layer):
        for which, source in enumerate((qw_ref, kw_ref, vw_ref)):
            turned = jnp.transpose(source[layer])
            for i in range(seqs):
                wt_ref[layer, i, which * head : (which + 1) * head, :] = turned[
                    i * head : (i + 1) * head, :
                ]

    @pl.when(inner)
    def _():
        sends(inner_plan, 0, "start")

    @pl.when(jnp.logical_not(inner))
    def _():
        sends(outer_plan, 0, "start")

    docs[s] = jnp.broadcast_to(docs_ref[...].astype(jnp.float32), docs.shape[1:])
    doc_c = [
        remote(docs.at[s], docs.at[s], (doc_send, doc_recv), o, o, {"sp": ahead(o)}) for o in hops
    ]
    for copy in doc_c:
        copy.start()
    for copy in loads[1:]:
        copy.wait()
    turn(0)

    @pl.when(inner)
    def _():
        sends(inner_plan, 1, "start")

    @pl.when(jnp.logical_not(inner))
    def _():
        for n in (1, 2):
            sends(outer_plan, n, "start")

    for layer in range(1, layers):
        turn(layer)

    @pl.when(jnp.logical_not(inner))
    def _():
        sends(outer_plan, 3, "start")

    for layer in range(layers):
        wo[layer, t, s] = woin_ref[layer]
    assert not started

    def project(layer, i):
        total = jnp.zeros((rows, 1), jnp.float32)
        for part in range(tps):
            piece = xg[layer, part, block_rows(i), :].astype(jnp.float32)
            total = total + jnp.sum(piece * piece, axis=1, keepdims=True)
        factor = lax.rsqrt(total * (1.0 / width) + epsilon)
        for part in range(tps):
            piece = xg[layer, part, block_rows(i), :].astype(jnp.float32)
            gain = ngain_ref[layer : layer + 1, part * cols : (part + 1) * cols]
            nb[:, part * cols : (part + 1) * cols] = (piece * factor * gain).astype(jnp.bfloat16)
        span = width // seqs
        raw = jnp.zeros((pair * 3 * head, rows), jnp.float32)
        for part in range(seqs):
            raw = raw + lax.dot_general(
                wq[layer, part].reshape(pair * 3 * head, span),
                nb[:, part * span : (part + 1) * span],
                (((1,), (1,)), ((), ())),
                preferred_element_type=jnp.float32,
            )

        def normal(value, gain):
            mean = jnp.mean(value * value, axis=0, keepdims=True)
            column = jnp.transpose(jnp.broadcast_to(gain, (128, head)))[:, 0:1]
            return value * lax.rsqrt(mean + epsilon) * column

        for a in range(pair):
            query, keys, values = [
                raw[(3 * a + n) * head : (3 * a + n + 1) * head] for n in range(3)
            ]
            query = normal(query, qgain_ref[layer : layer + 1, :]) * head ** (-0.5)
            keys = normal(keys, kgain_ref[layer : layer + 1, :])
            q_s[a, i] = query.astype(jnp.bfloat16)
            k_s[a, i] = jnp.transpose(keys).astype(jnp.bfloat16)
            v_s[a, i] = values.astype(jnp.bfloat16)

    def attend_block(j, a):
        pieces = []
        for i in range(max(0, j - depth), j + 1):
            score = jnp.dot(k_s[a, i], q_s[a, j], preferred_element_type=jnp.float32)
            same = dcol[i][:, 0:1] == docs[j, 0:1, :]
            pieces.append((i, jnp.where(same, score + bias[a, j - i], NEG)))
        peak = pieces[0][1].max(axis=0, keepdims=True)
        for _, piece in pieces[1:]:
            peak = jnp.maximum(peak, piece.max(axis=0, keepdims=True))
        mass = jnp.zeros((1, rows), jnp.float32)
        mixed = jnp.zeros((head, rows), jnp.float32)
        for i, piece in pieces:
            expo = jnp.exp(piece - peak)
            mass = mass + jnp.sum(expo, axis=0, keepdims=True)
            mixed = mixed + jnp.dot(
                v_s[a, i], expo.astype(jnp.bfloat16), preferred_element_type=jnp.float32
            )
        return (mixed / mass).astype(jnp.bfloat16)

    def out_product(layer, heads_all, held):
        return lax.dot_general(
            heads_all,
            wo[layer, held].reshape(-1, cols),
            (((0,), (0,)), ((), ())),
            preferred_element_type=jnp.float32,
        )

    def rest_copy(half, held):
        place = xg.at[1, held, block_rows(edge), :]
        return remote(place, place, (rs_send, rs_recv), half, half, {"sp": edge})

    def ag_copy(kind, n):
        place = ag.at[side if kind else t, n]
        index = (kind, n)
        where = {"tp": core if kind else side}
        return remote(place, place, (at_send, at_recv), index, index, where)

    def beside_copy():
        place = ag.at[t]
        return remote(place, place, (at_send, at_recv), (2, 0), (2, 0), {"tp": core})

    def last_copy(j):
        return remote(
            o_s.at[j], ag.at[t, inside], (az_send, az_recv), j, inside, {"sp": j}
        )

    @pl.when(inner)
    def _():
        other = seqs - 1 - s
        for part in range(tps):
            xg[0, part, block_rows(s), :] = x_ref[:, part * cols : (part + 1) * cols]
        for layer in range(layers):
            wq[layer, s] = wt_ref[layer, pl.ds(pair * inside, pair)]
        begin(o_whole(0))
        key_seg = lax.broadcasted_iota(jnp.int32, (rows, rows), 0) // SEG
        query_seg = lax.broadcasted_iota(jnp.int32, (rows, rows), 1) // SEG
        entries = (bias_ref.shape[1] - 1) // 128 * 128
        tables = []
        for a in range(pair):
            line = bias_ref[pl.ds(pair * inside + a, 1), :]
            line, final = line[:, :entries], line[:, entries:]
            tables.append(
                jnp.concatenate(
                    [line, jnp.broadcast_to(final, (1, (depth + 2) * rows - entries))], axis=1
                )
            )
        for d in range(depth + 1):
            gap = query_seg + (d * rows) // SEG - key_seg
            for a in range(pair):
                spread = jnp.broadcast_to(
                    tables[a][:, d * rows : (d + 2) * rows], (rows, 2 * rows)
                )
                rolled = pltpu.roll(spread, 0, 1, stride=1, stride_axis=0)
                bias[a, d] = jnp.where((gap >= 0) & (gap <= LEFT), rolled[:, rows:], NEG)
        order = [(block, h) for h in range(parts) for block in (edge, other)]
        fan(*order[0])
        fan(*order[1])
        for copy in doc_c:
            copy.wait_recv()
        for i in range(seqs):
            dcol[i] = jnp.transpose(jnp.broadcast_to(docs[i, 0:1, :], (128, rows)))
        pass_on(*order[0])
        fan(*order[2])
        fan(*order[3])
        pass_on(*order[1])
        spread_w(0, edge)
        spread_w(0, other)
        pass_on(*order[2])
        fan(beyond, 0)
        pass_on(*order[3])
        spread_w(0, beyond)
        sends(inner_plan, 2, "start")
        for h in range(1, parts):
            fan(beyond, h)
        pass_on(beyond, 0)
        for h in range(1, parts):
            pass_on(beyond, h)
        for block in (edge, other, beyond):
            w_relay(0, block).wait_recv()
        project(0, s)
        spread_o(0, other)
        for block in (edge, other, beyond):
            for h in range(parts):
                tp_copy(0, block, h).wait_recv()
                tp_copy(2, block, h).wait_recv()
            project(0, block)
            if block is edge:
                spread_o(0, edge, True)
            if block is other:
                spread_o(0, beyond)

        mid_z, mid_x, mid_c, new_c = {}, {}, {}, {}
        turns = (0, 3, 1, 2)
        for n, j in enumerate(turns):
            for a in range(pair):
                mids[j, t, inside, a * head : (a + 1) * head, :] = attend_block(j, a)
            place = mids.at[j, t, inside]
            mid_z[j] = send(place, place, (mz_send, mz_recv), j, {"sp": other})
            mid_x[j, 0] = send(place, place, (mx_send, mx_recv), (j, 0), {"tp": side})
            if n == 0:
                side_o(0, other)
            if n == 1:
                side_o(0, edge)
            if n == 2:
                spread_w(1, other)

        def mid_first(j):
            mid_z[j].wait_recv()
            place = mids.at[j, t, 1 - inside]
            mid_x[j, 1] = send(place, place, (mx_send, mx_recv), (j, 1), {"tp": side})
            place = mids.at[j, t]
            mid_c[j, 0] = send(place, place, (mc_send, mc_recv), (j, 0), {"tp": core})

        def mid_second(j):
            for n in range(2):
                mid_x[j, n].wait_recv()
            place = mids.at[j, side]
            mid_c[j, 1] = send(place, place, (mc_send, mc_recv), (j, 1), {"tp": core})

        def mid_third(j):
            for half in range(2):
                mid_c[j, half].wait_recv()
            heads_all = mids[j].reshape(tps * seqs * head, rows)
            for half, held in enumerate((t, side)):
                kept = xg[0, held, block_rows(j), :].astype(jnp.float32)
                place = xg.at[1, held, block_rows(j), :]
                place[...] = (kept + out_product(0, heads_all, held)).astype(jnp.bfloat16)
                new_c[j, half] = send(place, place, (nc_send, nc_recv), (j, half), {"tp": core})
                if j in (0, seqs - 1):

                    @pl.when(edge == j)
                    def _(half=half, held=held):
                        rest_copy(half, held).start()

        def mid_fourth(j):
            for half in range(2):
                new_c[j, half].wait_recv()
            project(1, j)

        mid_first(0)
        side_o(0, beyond)
        mid_first(3)
        mid_second(0)
        spread_w(1, beyond)
        mid_first(1)
        mid_second(3)
        mid_first(2)
        mid_second(1)
        mid_second(2)
        spread_w(1, edge)
        begin(o_whole(1))
        sends(inner_plan, 3, "start")
        ready_o(0, (other, beyond), (edge, other, beyond))
        mid_third(0)
        mid_third(3)
        spread_o(1, beyond)
        mid_third(1)
        w_relay(1, edge).wait_recv()
        for block in (other, beyond):
            w_relay(1, block).wait_recv()
        def finish(j):
            for a in range(pair):
                o_s[j, a * head : (a + 1) * head, :] = attend_block(j, a)

            @pl.when(s != j)
            def _():
                last_copy(j).start()

        mid_third(2)
        mid_fourth(0)
        finish(0)
        spread_o(1, other)
        mid_fourth(3)
        spread_o(1, edge, True)
        side_o(1, beyond)
        mid_fourth(1)
        finish(1)
        side_o(1, other)
        mid_fourth(2)
        finish(3)
        side_o(1, edge)
        finish(2)
        ag[t, inside] = o_s[s]
        begin(ag_copy(0, inside))
        ag_in = remote(o_s.at[0], ag.at[t, 1 - inside], (az_send, az_recv), s, 1 - inside, {"sp": other})
        ag_in.wait_recv()
        begin(ag_copy(0, 1 - inside))
        begin(beside_copy())
        ready_o(1, (other, beyond), (edge, other, beyond))
        for half, held in enumerate((t, side)):
            rest_copy(half, held).wait_send()
        for o in hops:
            last_copy(ahead(o)).wait_send()
        for n in range(4):
            sends(inner_plan, n, "wait_send")
        settle()

    @pl.when(jnp.logical_not(inner))
    def _():
        begin(o_whole(1))
        for copy in doc_c:
            copy.wait_recv()
        spread_o(1, near, True)
        for block in (seqs - 1 - s, far):
            spread_o(1, block)
        for o in hops:
            side_o(1, ahead(o))
        for half, held in enumerate((t, side)):
            rest_copy(half, held).wait_recv()
        for n in (inside, 1 - inside):
            place = ag.at[t, n]
            remote(place, place, (az_send, az_recv), s, n, {"sp": near}).wait_recv()
            begin(ag_copy(0, n))
        begin(beside_copy())
        ready_o(1, (far, seqs - 1 - s), (near, far, seqs - 1 - s))
        settle()
        for n in range(4):
            sends(outer_plan, n, "wait_send")

    for n in (inside, 1 - inside):
        ag_copy(0, n).wait_recv()
        begin(ag_copy(1, n))
    beside_copy().wait_recv()
    for n in (inside, 1 - inside):
        ag_copy(1, n).wait_recv()
    heads_all = ag[...].reshape(tps * seqs * head, rows)
    last = []
    for half, held in enumerate((t, side)):
        kept = xg[1, held, block_rows(s), :].astype(jnp.float32)
        fin[held] = (kept + out_product(1, heads_all, held)).astype(jnp.bfloat16)
        place = fin.at[held]
        last.append(send(place, place, (fn_send, fn_recv), half, {"tp": core}))
    for copy in last:
        copy.wait_recv()
    for part in range(tps):
        out_ref[:, part * cols : (part + 1) * cols] = fin[part]
    settle()
    for copy in doc_c:
        copy.wait_send()

def fused_device(
    sizes,
    stream,
    doc_ids,
    norm_gain,
    query_weight,
    key_weight,
    value_weight,
    out_weight,
    query_gain,
    key_gain,
    rel_bias,
):
    groups, seqs, tps = sizes
    rows, width = stream.shape
    cols = width // tps
    layers, deep, _ = query_weight.shape
    head = query_gain.shape[1]
    depth = -(-LEFT * SEG // rows)

    dma = pltpu.SemaphoreType.DMA
    bf16 = jnp.bfloat16
    pair = seqs // 2
    whole = [stream, query_weight, key_weight, value_weight, out_weight]
    scratch = [pltpu.VMEM(one.shape, one.dtype) for one in whole] + [dma((len(whole),))]
    scratch += [
        pltpu.VMEM((layers, seqs, 3 * head, deep), bf16),
        pltpu.VMEM((layers, tps, seqs * rows, cols), bf16),
        pltpu.VMEM((layers, seqs, pair, 3 * head, deep), bf16),
        pltpu.VMEM((layers, tps, seqs) + out_weight.shape[1:], bf16),
        pltpu.VMEM((seqs, 8, rows), jnp.float32),
        pltpu.VMEM((seqs, rows, 128), jnp.float32),
        pltpu.VMEM((seqs, tps, 2, pair * head, rows), bf16),
        pltpu.VMEM((tps, 2, pair * head, rows), bf16),
        pltpu.VMEM((tps, rows, cols), bf16),
        pltpu.VMEM((pair, depth + 1, rows, rows), jnp.float32),
        pltpu.VMEM((rows, width), bf16),
        pltpu.VMEM((pair, seqs, head, rows), bf16),
        pltpu.VMEM((pair, seqs, rows, head), bf16),
        pltpu.VMEM((pair, seqs, head, rows), bf16),
        pltpu.VMEM((seqs, pair * head, rows), bf16),
    ]
    pairs = [
        (seqs,),
        (seqs, 2),
        (3, seqs, 2),
        (layers, seqs),
        (layers, seqs),
        (layers, seqs),
        (layers, seqs),
        (layers, seqs),
        (layers, seqs),
        (seqs,),
        (seqs, 2),
        (seqs, 2),
        (seqs, 2),
        (2,),
        (seqs,),
        (3, 2),
        (2,),
    ]
    scratch += [dma(shape) for shape in pairs for _ in range(2)]
    return pl.pallas_call(
        functools.partial(fused_kernel, sizes),
        name="fused_layers",
        out_shape=jax.ShapeDtypeStruct((rows, width), bf16),
        in_specs=[
            pl.BlockSpec(memory_space=pltpu.HBM if n in (0, 3, 4, 5, 6) else pltpu.VMEM)
            for n in range(10)
        ],
        out_specs=pl.BlockSpec(memory_space=pltpu.VMEM),
        scratch_shapes=scratch,
        compiler_params=pltpu.CompilerParams(
            collective_id=0, has_side_effects=True, vmem_limit_bytes=58 * 1024 * 1024
        ),
    )(
        stream,
        doc_ids[None],
        norm_gain,
        query_weight,
        key_weight,
        value_weight,
        out_weight,
        query_gain,
        key_gain,
        rel_bias,
    )


def solution(mesh):
    placed = (
        P(("grp", "sp"), None),
        P(("grp", "sp")),
        P(),
        P(None, "sp", "tp"),
        P(None, "sp", "tp"),
        P(None, "sp", "tp"),
        P(None, "sp", "tp"),
        P(),
        P(),
        P("tp", None),
    )
    sizes = tuple(mesh.shape[axis] for axis in ("grp", "sp", "tp"))

    def body(*args):
        one_head_each = args[-1].shape[0] == sizes[1]
        fits = sizes == (2, 4, 4) and args[0].shape[0] == MAXREL
        if one_head_each and fits:
            return fused_device(sizes, *args)
        return on_device(*args)

    return jax.shard_map(
        body, mesh=mesh, in_specs=placed, out_specs=P(("grp", "sp"), None), check_vma=False
    )
```

```python
import functools

import jax
import jax.numpy as jnp
from jax import lax
from jax.experimental import pallas as pl
from jax.experimental.pallas import tpu as pltpu
from jax.sharding import PartitionSpec as P

SEG = 64
LEFT = 8
MAXREL = 256
LAYERS = 2


epsilon = 1e-06


def shifted(value, axis, steps):
    count = lax.axis_size(axis)
    initial, last = (max(0, -steps), min(count, count - steps))
    return lax.ppermute(value, axis, [(source, source + steps) for source in range(initial, last)])


def row_norm(values, gain):
    return values * lax.rsqrt(jnp.mean(values * values, axis=-1, keepdims=True) + epsilon) * gain


def bias_table(rel_bias):
    heads_here = rel_bias.shape[0]
    reach = LEFT * SEG
    width = (LEFT + 1) * SEG
    highest = reach + SEG - 1
    reversed_bias = rel_bias[:, ::-1]
    upper_fill = jnp.broadcast_to(rel_bias[:, -1:], (heads_here, highest - MAXREL))
    flat_row = jnp.concatenate([upper_fill, reversed_bias[:, : MAXREL + SEG]], axis=1)
    lines = [
        flat_row[:, SEG - 1 - position : SEG - 1 - position + width] for position in range(SEG)
    ]
    return jnp.stack(lines, axis=1)


def attend(query, ext_keys, ext_values, ext_docs, own_docs, offset, table):
    rows, heads_here, head_size = query.shape
    count = rows // SEG
    width = (LEFT + 1) * SEG
    blocks = query.reshape(count, SEG, heads_here, head_size)
    key_blocks = ext_keys.reshape(count + LEFT, SEG, heads_here, head_size)
    value_blocks = ext_values.reshape(count + LEFT, SEG, heads_here, head_size)
    doc_blocks = ext_docs.reshape(count + LEFT, SEG)
    score_parts = [
        jnp.einsum(
            "nqhd,nkhd->nhqk",
            blocks,
            key_blocks[earlier : earlier + count],
            preferred_element_type=jnp.float32,
        )
        for earlier in range(LEFT + 1)
    ]
    scores = jnp.concatenate(score_parts, axis=-1)
    scores = scores * head_size ** (-0.5) + table[None]
    doc_band = jnp.concatenate(
        [doc_blocks[earlier : earlier + count] for earlier in range(LEFT + 1)], axis=1
    )
    key_pos = (
        offset
        + SEG * jnp.arange(count, dtype=jnp.int32)[:, None]
        - LEFT * SEG
        + jnp.arange(width, dtype=jnp.int32)[None, :]
    )
    allowed = (key_pos >= 0)[:, None, None, :] & (
        doc_band[:, None, None, :] == own_docs.reshape(count, SEG)[:, None, :, None]
    )
    scores = jnp.where(allowed, scores, -1e30)
    peak = jnp.max(scores, axis=-1, keepdims=True)
    expo = jnp.exp(scores - peak)
    weights = (expo / jnp.sum(expo, axis=-1, keepdims=True)).astype(jnp.bfloat16)
    mixed = jnp.zeros((count, SEG, heads_here, head_size), jnp.float32)
    for earlier in range(LEFT + 1):
        part_weights = weights[..., earlier * SEG : (earlier + 1) * SEG]
        mixed = mixed + jnp.einsum(
            "nhqk,nkhd->nqhd",
            part_weights,
            value_blocks[earlier : earlier + count],
            preferred_element_type=jnp.float32,
        )
    return mixed.astype(jnp.bfloat16).reshape(rows, heads_here * head_size)


def on_device(
    stream,
    doc_ids,
    norm_gain,
    query_weight,
    key_weight,
    value_weight,
    out_weight,
    query_gain,
    key_gain,
    rel_bias,
):
    rows = stream.shape[0]
    heads_here = rel_bias.shape[0]
    head_size = query_gain.shape[1]
    local_width = heads_here * head_size
    reach = LEFT * SEG
    depth = -(-reach // rows)
    offset = lax.axis_index("sp") * rows
    col_width = out_weight.shape[2]
    col_start = lax.axis_index("tp") * col_width
    table = bias_table(rel_bias)
    x = stream
    for layer in range(LAYERS):
        widened = x.astype(jnp.float32)
        normed = row_norm(widened, norm_gain[layer]).astype(jnp.bfloat16)
        own_cols = normed
        q_raw = jnp.dot(
            own_cols,
            lax.all_gather(query_weight[layer], "sp", axis=0, tiled=True),
            preferred_element_type=jnp.float32,
        )
        k_raw = jnp.dot(
            normed,
            lax.all_gather(key_weight[layer], "sp", axis=0, tiled=True),
            preferred_element_type=jnp.float32,
        )
        v_raw = jnp.dot(
            normed,
            lax.all_gather(value_weight[layer], "sp", axis=0, tiled=True),
            preferred_element_type=jnp.float32,
        )
        query = row_norm(q_raw.reshape(rows, heads_here, head_size), query_gain[layer]).astype(
            jnp.bfloat16
        )
        keys = row_norm(
            k_raw.reshape(normed.shape[0], heads_here, head_size), key_gain[layer]
        ).astype(jnp.bfloat16)
        values = v_raw.astype(jnp.bfloat16)
        flat_keys = keys.reshape(rows, local_width)
        tail = (flat_keys, values, doc_ids)
        received = [
            shifted((tail[0], tail[1], tail[2]), "sp", distance_back)
            for distance_back in range(depth, 0, -1)
        ]
        ext_keys = jnp.concatenate([item[0] for item in received] + [flat_keys], axis=0)
        ext_values = jnp.concatenate([item[1] for item in received] + [values], axis=0)
        ext_docs = jnp.concatenate([item[2] for item in received] + [doc_ids], axis=0)
        ext_keys = ext_keys.reshape(reach + rows, heads_here, head_size)
        ext_values = ext_values.reshape(reach + rows, heads_here, head_size)
        attended = attend(query, ext_keys, ext_values, ext_docs, doc_ids, offset, table)
        all_heads = lax.all_gather(attended, "tp", axis=1, tiled=True)
        projected = jnp.dot(
            all_heads,
            lax.all_gather(out_weight[layer], "sp", axis=0, tiled=True),
            preferred_element_type=jnp.float32,
        )
        own_cols = lax.dynamic_slice_in_dim(widened, col_start, col_width, 1)
        new_cols = (own_cols + projected).astype(jnp.bfloat16)
        x = lax.all_gather(new_cols, "tp", axis=1, tiled=True)
    return x


MESH = pl.DeviceIdType.MESH
NEG = -1e30


def fused_kernel(
    sizes,
    x_in,
    docs_ref,
    ngain_ref,
    qw_in,
    kw_in,
    vw_in,
    wo_in,
    qgain_ref,
    kgain_ref,
    bias_ref,
    out_ref,
    x_ref,
    qw_ref,
    kw_ref,
    vw_ref,
    woin_ref,
    load,
    save,
    wt_ref,
    xg,
    wq,
    wo,
    docs,
    dcol,
    mids,
    ag,
    fin,
    bias,
    masked,
    nb,
    q_s,
    k_s,
    v_s,
    o_s,
    doc_send,
    doc_recv,
    xz_send,
    xz_recv,
    xt_send,
    xt_recv,
    wz_send,
    wz_recv,
    wy_send,
    wy_recv,
    oz_send,
    oz_recv,
    ox_send,
    ox_recv,
    oy_send,
    oy_recv,
    op_send,
    op_recv,
    mz_send,
    mz_recv,
    mx_send,
    mx_recv,
    mc_send,
    mc_recv,
    nc_send,
    nc_recv,
    rs_send,
    rs_recv,
    az_send,
    az_recv,
    at_send,
    at_recv,
    fn_send,
    fn_recv,
):
    groups, seqs, tps = sizes
    rows, width = x_ref.shape
    cols = width // tps
    head = qgain_ref.shape[1]
    layers = wt_ref.shape[0]
    depth = bias.shape[1] - 1
    parts = xz_send.shape[1]
    tall = rows // parts
    pair = bias.shape[0]
    grp = lax.axis_index("grp")
    s = lax.axis_index("sp")
    t = lax.axis_index("tp")
    other_grp = 1 - grp
    core = t + 1 - 2 * lax.rem(t, 2)
    side = lax.rem(t + 2, tps)
    inner = (s > 0) & (s < seqs - 1)
    near = jnp.clip(s, 1, seqs - 2)
    far = seqs - 1 - near
    first = jnp.where(inner, seqs - 1 - s, near)
    inside = near - 1
    edge = jnp.where(near == 1, 0, seqs - 1)
    beyond = seqs - 1 - edge
    started = []

    def remote(src, dst, sems, out_index, in_index, where):
        return pltpu.make_async_remote_copy(
            src_ref=src,
            dst_ref=dst,
            send_sem=sems[0].at[out_index],
            recv_sem=sems[1].at[in_index],
            device_id=where,
            device_id_type=MESH,
        )

    def send(src, dst, sems, index, where):
        copy = remote(src, dst, sems, index, index, where)
        copy.start()
        started.append(copy)
        return copy

    def settle():
        for copy in started:
            copy.wait_send()
        started.clear()

    def ahead(o):
        return lax.rem(s + o, seqs)

    def block_rows(i):
        return pl.ds(pl.multiple_of(i * rows, rows), rows)

    def cut_rows(i, h):
        return pl.ds(pl.multiple_of(i * rows + h * tall, tall), tall)

    loads = [
        pltpu.make_async_copy(src, dst, load.at[n])
        for n, (src, dst) in enumerate(
            zip((x_in, qw_in, kw_in, vw_in, wo_in), (x_ref, qw_ref, kw_ref, vw_ref, woin_ref))
        )
    ]
    for copy in loads:
        copy.start()
    barrier = pltpu.get_barrier_semaphore()
    partners = [{"sp": ahead(o)} for o in range(1, seqs)]
    partners += [{"tp": core}, {"tp": side}, {"grp": other_grp}]
    for where in partners:
        pl.semaphore_signal(barrier, inc=1, device_id=where, device_id_type=MESH)
    pl.semaphore_wait(barrier, len(partners))
    loads[0].wait()

    own_cols = pl.ds(pl.multiple_of(t * cols, cols), cols)
    ohalf = woin_ref.shape[1] // 2
    opart = pl.ds(pl.multiple_of(grp * ohalf, ohalf), ohalf)
    hops = list(range(1, seqs))

    def x_copy(source, dest, h):
        place = xg.at[0, t, cut_rows(source, h), :]
        return remote(
            x_ref.at[h * tall : (h + 1) * tall, own_cols],
            place,
            (xz_send, xz_recv),
            (dest, h),
            (source, h),
            {"sp": dest},
        )

    def w_copy(layer, source, dest):
        return remote(
            wt_ref.at[layer, pair * (dest - 1) + grp],
            wq.at[layer, source, grp],
            (wz_send, wz_recv),
            (layer, dest),
            (layer, source),
            {"sp": dest},
        )

    def o_copy(layer, source, dest):
        return remote(
            woin_ref.at[layer, opart, :],
            wo.at[layer, t, source, opart, :],
            (oz_send, oz_recv),
            (layer, dest),
            (layer, source),
            {"sp": dest},
        )

    def w_full(layer, source, dest):
        return remote(
            wt_ref.at[layer, pl.ds(pair * (dest - 1), pair)],
            wq.at[layer, source],
            (wz_send, wz_recv),
            (layer, dest),
            (layer, source),
            {"sp": dest},
        )

    def o_full(layer, source, dest):
        return remote(
            woin_ref.at[layer],
            wo.at[layer, t, source],
            (oz_send, oz_recv),
            (layer, dest),
            (layer, source),
            {"sp": dest},
        )

    def outer_plan(n):
        if n == 0:
            return [x_copy(s, near, h) for h in range(parts)]
        if n == 1:
            x_far = [x_copy(s, far, h) for h in range(parts)]
            return [w_copy(0, s, near)] + x_far + [w_copy(0, s, far)]
        if n == 2:
            return [o_copy(0, s, far), o_full(0, s, near)]
        plan = [w_copy(1, s, near), w_copy(1, s, far)]
        return plan + [o_copy(1, s, far), o_full(1, s, near), o_copy(1, s, seqs - 1 - s)]

    def inner_plan(n):
        other = seqs - 1 - s
        if n == 0:
            return [x_copy(s, other, h) for h in range(parts)]
        if n == 1:
            return [w_copy(0, s, other), o_full(1, s, edge)]
        if n == 2:
            return [o_copy(0, s, other), w_copy(1, s, other)]
        return [o_copy(1, s, other), o_copy(1, s, beyond)]

    def sends(plan, n, act):
        for copy in plan(n):
            getattr(copy, act)()

    def tp_copy(kind, block, h):
        held = side if kind == 2 else t
        place = xg.at[0, held, cut_rows(block, h), :]
        index = (kind, block, h)
        where = {"tp": side if kind == 1 else core}
        return remote(place, place, (xt_send, xt_recv), index, index, where)

    def w_relay(layer, block):
        place = wq.at[layer, block, grp]
        index = (layer, block)
        return remote(place, place, (wy_send, wy_recv), index, index, {"grp": other_grp})

    def o_relay(layer, kind, block):
        held = side if kind == 2 else t
        place = wo.at[layer, held, block, opart, :]
        sems = ((ox_send, ox_recv), (oy_send, oy_recv), (op_send, op_recv))[kind]
        index = (layer, block)
        where = {"tp": side} if kind == 0 else {"grp": other_grp}
        return remote(place, place, sems, index, index, where)

    def o_whole(layer):
        place = wo.at[layer, t, s]
        index = (layer, s)
        return remote(woin_ref.at[layer], place, (ox_send, ox_recv), index, index, {"tp": side})

    def begin(copy):
        copy.start()
        started.append(copy)

    def fan(block, h):
        x_copy(block, near, h).wait_recv()
        begin(tp_copy(1, block, h))
        begin(tp_copy(0, block, h))

    def pass_on(block, h):
        tp_copy(1, block, h).wait_recv()
        begin(tp_copy(2, block, h))

    def spread_w(layer, block):
        w_copy(layer, block, near).wait_recv()
        begin(w_relay(layer, block))

    def spread_o(layer, block, whole=False):
        (o_full(layer, block, near) if whole else o_copy(layer, block, near)).wait_recv()
        begin(o_relay(layer, 0, block))
        if not whole:
            begin(o_relay(layer, 1, block))

    def side_o(layer, block):
        o_relay(layer, 0, block).wait_recv()
        begin(o_relay(layer, 2, block))

    def ready_own(layer, relayed):
        for block in relayed:
            o_relay(layer, 1, block).wait_recv()

    def ready_side(layer, sides):
        o_whole(layer).wait_recv()
        for block in sides:
            o_relay(layer, 2, block).wait_recv()

    def ready_o(layer, relayed, sides):
        ready_own(layer, relayed)
        ready_side(layer, sides)

    def turn(layer):
        for which, source in enumerate((qw_ref, kw_ref, vw_ref)):
            turned = jnp.transpose(source[layer])
            for i in range(seqs):
                wt_ref[layer, i, which * head : (which + 1) * head, :] = turned[
                    i * head : (i + 1) * head, :
                ]

    @pl.when(inner)
    def _():
        sends(inner_plan, 0, "start")

    @pl.when(jnp.logical_not(inner))
    def _():
        sends(outer_plan, 0, "start")

    docs[s] = jnp.broadcast_to(docs_ref[...].astype(jnp.float32), docs.shape[1:])
    doc_c = [
        remote(docs.at[s], docs.at[s], (doc_send, doc_recv), o, o, {"sp": ahead(o)}) for o in hops
    ]
    for copy in doc_c:
        copy.start()
    for copy in loads[1:]:
        copy.wait()
    turn(0)

    @pl.when(inner)
    def _():
        sends(inner_plan, 1, "start")

    @pl.when(jnp.logical_not(inner))
    def _():
        for n in (1, 2):
            sends(outer_plan, n, "start")

    for layer in range(1, layers):
        turn(layer)

    @pl.when(jnp.logical_not(inner))
    def _():
        sends(outer_plan, 3, "start")

    for layer in range(layers):
        wo[layer, t, s] = woin_ref[layer]
    assert not started

    def project(layer, i):
        total = jnp.zeros((rows, 1), jnp.float32)
        for part in range(tps):
            piece = xg[layer, part, block_rows(i), :].astype(jnp.float32)
            total = total + jnp.sum(piece * piece, axis=1, keepdims=True)
        factor = lax.rsqrt(total * (1.0 / width) + epsilon)
        for part in range(tps):
            piece = xg[layer, part, block_rows(i), :].astype(jnp.float32)
            gain = ngain_ref[layer : layer + 1, part * cols : (part + 1) * cols]
            nb[:, part * cols : (part + 1) * cols] = (piece * factor * gain).astype(jnp.bfloat16)
        span = width // seqs
        raw = jnp.zeros((pair * 3 * head, rows), jnp.float32)
        for part in range(seqs):
            raw = raw + lax.dot_general(
                wq[layer, part].reshape(pair * 3 * head, span),
                nb[:, part * span : (part + 1) * span],
                (((1,), (1,)), ((), ())),
                preferred_element_type=jnp.float32,
            )

        def normal(value, gain):
            mean = jnp.mean(value * value, axis=0, keepdims=True)
            column = jnp.transpose(jnp.broadcast_to(gain, (128, head)))[:, 0:1]
            return value * lax.rsqrt(mean + epsilon) * column

        for a in range(pair):
            query, keys, values = [
                raw[(3 * a + n) * head : (3 * a + n + 1) * head] for n in range(3)
            ]
            query = normal(query, qgain_ref[layer : layer + 1, :]) * head ** (-0.5)
            keys = normal(keys, kgain_ref[layer : layer + 1, :])
            q_s[a, i] = query.astype(jnp.bfloat16)
            k_s[a, i] = jnp.transpose(keys).astype(jnp.bfloat16)
            v_s[a, i] = values.astype(jnp.bfloat16)

    links = [(i, j) for j in range(seqs) for i in range(max(0, j - depth), j + 1)]

    def mask(a):
        for n, (i, j) in enumerate(links):
            same = dcol[i][:, 0:1] == docs[j, 0:1, :]
            masked[a, n] = jnp.where(same, bias[a, j - i], NEG)

    def attend_block(j, a):
        pieces = []
        for i in range(max(0, j - depth), j + 1):
            score = jnp.dot(k_s[a, i], q_s[a, j], preferred_element_type=jnp.float32)
            pieces.append((i, score + masked[a, links.index((i, j))]))
        peak = pieces[0][1].max(axis=0, keepdims=True)
        for _, piece in pieces[1:]:
            peak = jnp.maximum(peak, piece.max(axis=0, keepdims=True))
        mass = jnp.zeros((1, rows), jnp.float32)
        mixed = jnp.zeros((head, rows), jnp.float32)
        for i, piece in pieces:
            expo = jnp.exp(piece - peak)
            mass = mass + jnp.sum(expo, axis=0, keepdims=True)
            mixed = mixed + jnp.dot(
                v_s[a, i], expo.astype(jnp.bfloat16), preferred_element_type=jnp.float32
            )
        return (mixed / mass).astype(jnp.bfloat16)

    def out_product(layer, heads_all, held):
        return lax.dot_general(
            heads_all,
            wo[layer, held].reshape(-1, cols),
            (((0,), (0,)), ((), ())),
            preferred_element_type=jnp.float32,
        )

    def rest_copy(half, held):
        place = xg.at[1, held, block_rows(edge), :]
        return remote(place, place, (rs_send, rs_recv), half, half, {"sp": edge})

    def ag_copy(kind, n):
        place = ag.at[side if kind else t, n]
        index = (kind, n)
        where = {"tp": core if kind else side}
        return remote(place, place, (at_send, at_recv), index, index, where)

    def beside_copy():
        place = ag.at[t]
        return remote(place, place, (at_send, at_recv), (2, 0), (2, 0), {"tp": core})

    def last_copy(j):
        return remote(
            o_s.at[j], ag.at[t, inside], (az_send, az_recv), j, inside, {"sp": j}
        )

    @pl.when(inner)
    def _():
        other = seqs - 1 - s
        for part in range(tps):
            xg[0, part, block_rows(s), :] = x_ref[:, part * cols : (part + 1) * cols]
        for layer in range(layers):
            wq[layer, s] = wt_ref[layer, pl.ds(pair * inside, pair)]
        begin(o_whole(0))
        key_seg = lax.broadcasted_iota(jnp.int32, (rows, rows), 0) // SEG
        query_seg = lax.broadcasted_iota(jnp.int32, (rows, rows), 1) // SEG
        entries = (bias_ref.shape[1] - 1) // 128 * 128
        tables = []
        for a in range(pair):
            line = bias_ref[pl.ds(pair * inside + a, 1), :]
            line, final = line[:, :entries], line[:, entries:]
            tables.append(
                jnp.concatenate(
                    [line, jnp.broadcast_to(final, (1, (depth + 2) * rows - entries))], axis=1
                )
            )
        for d in range(depth + 1):
            gap = query_seg + (d * rows) // SEG - key_seg
            for a in range(pair):
                spread = jnp.broadcast_to(
                    tables[a][:, d * rows : (d + 2) * rows], (rows, 2 * rows)
                )
                rolled = pltpu.roll(spread, 0, 1, stride=1, stride_axis=0)
                bias[a, d] = jnp.where((gap >= 0) & (gap <= LEFT), rolled[:, rows:], NEG)
        order = [(block, h) for h in range(parts) for block in (edge, other)]
        fan(*order[0])
        fan(*order[1])
        for copy in doc_c:
            copy.wait_recv()
        for i in range(seqs):
            dcol[i] = jnp.transpose(jnp.broadcast_to(docs[i, 0:1, :], (128, rows)))
        mask(0)
        pass_on(*order[0])
        fan(*order[2])
        fan(*order[3])
        pass_on(*order[1])
        spread_w(0, edge)
        spread_w(0, other)
        mask(1)
        pass_on(*order[2])
        fan(beyond, 0)
        pass_on(*order[3])
        spread_w(0, beyond)
        sends(inner_plan, 2, "start")
        for h in range(1, parts):
            fan(beyond, h)
        pass_on(beyond, 0)
        for h in range(1, parts):
            pass_on(beyond, h)
        for block in (edge, other, beyond):
            w_relay(0, block).wait_recv()
        project(0, s)
        spread_o(0, other)
        for block in (edge, other, beyond):
            for h in range(parts):
                tp_copy(0, block, h).wait_recv()
                tp_copy(2, block, h).wait_recv()
            project(0, block)
            if block is edge:
                spread_o(0, edge, True)
            if block is other:
                spread_o(0, beyond)

        mid_z, mid_x, mid_c, new_c = {}, {}, {}, {}
        turns = (0, 3, 1, 2)
        for n, j in enumerate(turns):
            for a in range(pair):
                mids[j, t, inside, a * head : (a + 1) * head, :] = attend_block(j, a)
            place = mids.at[j, t, inside]
            mid_z[j] = send(place, place, (mz_send, mz_recv), j, {"sp": other})
            mid_x[j, 0] = send(place, place, (mx_send, mx_recv), (j, 0), {"tp": side})
            if n == 0:
                side_o(0, other)
            if n == 1:
                side_o(0, edge)
            if n == 2:
                spread_w(1, other)

        def mid_first(j):
            mid_z[j].wait_recv()
            place = mids.at[j, t, 1 - inside]
            mid_x[j, 1] = send(place, place, (mx_send, mx_recv), (j, 1), {"tp": side})
            place = mids.at[j, t]
            mid_c[j, 0] = send(place, place, (mc_send, mc_recv), (j, 0), {"tp": core})

        def mid_second(j):
            for n in range(2):
                mid_x[j, n].wait_recv()
            place = mids.at[j, side]
            mid_c[j, 1] = send(place, place, (mc_send, mc_recv), (j, 1), {"tp": core})

        def mid_third(j, half):
            if half == 0:
                for n in range(2):
                    mid_c[j, n].wait_recv()
            held = side if half else t
            heads_all = mids[j].reshape(tps * seqs * head, rows)
            kept = xg[0, held, block_rows(j), :].astype(jnp.float32)
            place = xg.at[1, held, block_rows(j), :]
            place[...] = (kept + out_product(0, heads_all, held)).astype(jnp.bfloat16)
            new_c[j, half] = send(place, place, (nc_send, nc_recv), (j, half), {"tp": core})
            if j in (0, seqs - 1):

                @pl.when(edge == j)
                def _():
                    rest_copy(half, held).start()

        def mid_fourth(j):
            for half in range(2):
                new_c[j, half].wait_recv()
            project(1, j)

        mid_first(0)
        side_o(0, beyond)
        mid_first(3)
        mid_second(0)
        spread_w(1, beyond)
        mid_first(1)
        mid_second(3)
        mid_first(2)
        mid_second(1)
        mid_second(2)
        spread_w(1, edge)
        begin(o_whole(1))
        sends(inner_plan, 3, "start")
        ready_own(0, (other, beyond))
        mid_third(0, 0)
        mid_third(3, 0)
        ready_side(0, (edge, other, beyond))
        mid_third(0, 1)
        mid_third(3, 1)
        spread_o(1, beyond)
        mid_third(1, 0)
        mid_third(1, 1)
        w_relay(1, edge).wait_recv()
        for block in (other, beyond):
            w_relay(1, block).wait_recv()
        def finish(j):
            for a in range(pair):
                o_s[j, a * head : (a + 1) * head, :] = attend_block(j, a)

            @pl.when(s != j)
            def _():
                last_copy(j).start()

        mid_third(2, 0)
        mid_third(2, 1)
        mid_fourth(0)
        finish(0)
        spread_o(1, other)
        mid_fourth(3)
        spread_o(1, edge, True)
        side_o(1, beyond)
        mid_fourth(1)
        finish(1)
        side_o(1, other)
        mid_fourth(2)
        finish(3)
        side_o(1, edge)
        finish(2)
        ag[t, inside] = o_s[s]
        begin(ag_copy(0, inside))
        ag_in = remote(o_s.at[0], ag.at[t, 1 - inside], (az_send, az_recv), s, 1 - inside, {"sp": other})
        ag_in.wait_recv()
        begin(ag_copy(0, 1 - inside))
        begin(beside_copy())
        ready_o(1, (other, beyond), (edge, other, beyond))
        for half, held in enumerate((t, side)):
            rest_copy(half, held).wait_send()
        for o in hops:
            last_copy(ahead(o)).wait_send()
        for n in range(4):
            sends(inner_plan, n, "wait_send")
        settle()

    @pl.when(jnp.logical_not(inner))
    def _():
        begin(o_whole(1))
        for copy in doc_c:
            copy.wait_recv()
        spread_o(1, near, True)
        for block in (seqs - 1 - s, far):
            spread_o(1, block)
        for o in hops:
            side_o(1, ahead(o))
        for half, held in enumerate((t, side)):
            rest_copy(half, held).wait_recv()
        for n in (inside, 1 - inside):
            place = ag.at[t, n]
            remote(place, place, (az_send, az_recv), s, n, {"sp": near}).wait_recv()
            begin(ag_copy(0, n))
        begin(beside_copy())
        ready_o(1, (far, seqs - 1 - s), (near, far, seqs - 1 - s))
        settle()
        for n in range(4):
            sends(outer_plan, n, "wait_send")

    for n in (inside, 1 - inside):
        ag_copy(0, n).wait_recv()
        begin(ag_copy(1, n))
    beside_copy().wait_recv()
    for n in (inside, 1 - inside):
        ag_copy(1, n).wait_recv()
    heads_all = ag[...].reshape(tps * seqs * head, rows)
    last, stores = [], []

    def store(part):
        place = out_ref.at[:, pl.ds(pl.multiple_of(part * cols, cols), cols)]
        return pltpu.make_async_copy(fin.at[part], place, save.at[part])

    for half, held in enumerate((t, side)):
        kept = xg[1, held, block_rows(s), :].astype(jnp.float32)
        fin[held] = (kept + out_product(1, heads_all, held)).astype(jnp.bfloat16)
        place = fin.at[held]
        last.append(send(place, place, (fn_send, fn_recv), half, {"tp": core}))
        stores.append(store(held))
        stores[-1].start()
    for copy, held in zip(last, (core, lax.rem(core + 2, tps))):
        copy.wait_recv()
        stores.append(store(held))
        stores[-1].start()
    settle()
    for copy in doc_c:
        copy.wait_send()
    for copy in stores:
        copy.wait()

def fused_device(
    sizes,
    stream,
    doc_ids,
    norm_gain,
    query_weight,
    key_weight,
    value_weight,
    out_weight,
    query_gain,
    key_gain,
    rel_bias,
):
    groups, seqs, tps = sizes
    rows, width = stream.shape
    cols = width // tps
    layers, deep, _ = query_weight.shape
    head = query_gain.shape[1]
    depth = -(-LEFT * SEG // rows)

    dma = pltpu.SemaphoreType.DMA
    bf16 = jnp.bfloat16
    pair = seqs // 2
    links = sum(min(j, depth) + 1 for j in range(seqs))
    whole = [stream, query_weight, key_weight, value_weight, out_weight]
    scratch = [pltpu.VMEM(one.shape, one.dtype) for one in whole] + [dma((len(whole),)), dma((tps,))]
    scratch += [
        pltpu.VMEM((layers, seqs, 3 * head, deep), bf16),
        pltpu.VMEM((layers, tps, seqs * rows, cols), bf16),
        pltpu.VMEM((layers, seqs, pair, 3 * head, deep), bf16),
        pltpu.VMEM((layers, tps, seqs) + out_weight.shape[1:], bf16),
        pltpu.VMEM((seqs, 8, rows), jnp.float32),
        pltpu.VMEM((seqs, rows, 128), jnp.float32),
        pltpu.VMEM((seqs, tps, 2, pair * head, rows), bf16),
        pltpu.VMEM((tps, 2, pair * head, rows), bf16),
        pltpu.VMEM((tps, rows, cols), bf16),
        pltpu.VMEM((pair, depth + 1, rows, rows), jnp.float32),
        pltpu.VMEM((pair, links, rows, rows), jnp.float32),
        pltpu.VMEM((rows, width), bf16),
        pltpu.VMEM((pair, seqs, head, rows), bf16),
        pltpu.VMEM((pair, seqs, rows, head), bf16),
        pltpu.VMEM((pair, seqs, head, rows), bf16),
        pltpu.VMEM((seqs, pair * head, rows), bf16),
    ]
    pairs = [
        (seqs,),
        (seqs, 2),
        (3, seqs, 2),
        (layers, seqs),
        (layers, seqs),
        (layers, seqs),
        (layers, seqs),
        (layers, seqs),
        (layers, seqs),
        (seqs,),
        (seqs, 2),
        (seqs, 2),
        (seqs, 2),
        (2,),
        (seqs,),
        (3, 2),
        (2,),
    ]
    scratch += [dma(shape) for shape in pairs for _ in range(2)]
    return pl.pallas_call(
        functools.partial(fused_kernel, sizes),
        name="fused_layers",
        out_shape=jax.ShapeDtypeStruct((rows, width), bf16),
        in_specs=[
            pl.BlockSpec(memory_space=pltpu.HBM if n in (0, 3, 4, 5, 6) else pltpu.VMEM)
            for n in range(10)
        ],
        out_specs=pl.BlockSpec(memory_space=pl.ANY),
        scratch_shapes=scratch,
        compiler_params=pltpu.CompilerParams(
            collective_id=0, has_side_effects=True, vmem_limit_bytes=58 * 1024 * 1024
        ),
    )(
        stream,
        doc_ids[None],
        norm_gain,
        query_weight,
        key_weight,
        value_weight,
        out_weight,
        query_gain,
        key_gain,
        rel_bias,
    )


def solution(mesh):
    placed = (
        P(("grp", "sp"), None),
        P(("grp", "sp")),
        P(),
        P(None, "sp", "tp"),
        P(None, "sp", "tp"),
        P(None, "sp", "tp"),
        P(None, "sp", "tp"),
        P(),
        P(),
        P("tp", None),
    )
    sizes = tuple(mesh.shape[axis] for axis in ("grp", "sp", "tp"))

    def body(*args):
        one_head_each = args[-1].shape[0] == sizes[1]
        fits = sizes == (2, 4, 4) and args[0].shape[0] == MAXREL
        if one_head_each and fits:
            return fused_device(sizes, *args)
        return on_device(*args)

    return jax.shard_map(
        body, mesh=mesh, in_specs=placed, out_specs=P(("grp", "sp"), None), check_vma=False
    )
```

```python
import functools

import jax
import jax.numpy as jnp
from jax import lax
from jax.experimental import pallas as pl
from jax.experimental.pallas import tpu as pltpu
from jax.sharding import PartitionSpec as P

SEG = 64
LEFT = 8
MAXREL = 256
LAYERS = 2


epsilon = 1e-06


def shifted(value, axis, steps):
    count = lax.axis_size(axis)
    initial, last = (max(0, -steps), min(count, count - steps))
    return lax.ppermute(value, axis, [(source, source + steps) for source in range(initial, last)])


def row_norm(values, gain):
    return values * lax.rsqrt(jnp.mean(values * values, axis=-1, keepdims=True) + epsilon) * gain


def bias_table(rel_bias):
    heads_here = rel_bias.shape[0]
    reach = LEFT * SEG
    width = (LEFT + 1) * SEG
    highest = reach + SEG - 1
    reversed_bias = rel_bias[:, ::-1]
    upper_fill = jnp.broadcast_to(rel_bias[:, -1:], (heads_here, highest - MAXREL))
    flat_row = jnp.concatenate([upper_fill, reversed_bias[:, : MAXREL + SEG]], axis=1)
    lines = [
        flat_row[:, SEG - 1 - position : SEG - 1 - position + width] for position in range(SEG)
    ]
    return jnp.stack(lines, axis=1)


def attend(query, ext_keys, ext_values, ext_docs, own_docs, offset, table):
    rows, heads_here, head_size = query.shape
    count = rows // SEG
    width = (LEFT + 1) * SEG
    blocks = query.reshape(count, SEG, heads_here, head_size)
    key_blocks = ext_keys.reshape(count + LEFT, SEG, heads_here, head_size)
    value_blocks = ext_values.reshape(count + LEFT, SEG, heads_here, head_size)
    doc_blocks = ext_docs.reshape(count + LEFT, SEG)
    score_parts = [
        jnp.einsum(
            "nqhd,nkhd->nhqk",
            blocks,
            key_blocks[earlier : earlier + count],
            preferred_element_type=jnp.float32,
        )
        for earlier in range(LEFT + 1)
    ]
    scores = jnp.concatenate(score_parts, axis=-1)
    scores = scores * head_size ** (-0.5) + table[None]
    doc_band = jnp.concatenate(
        [doc_blocks[earlier : earlier + count] for earlier in range(LEFT + 1)], axis=1
    )
    key_pos = (
        offset
        + SEG * jnp.arange(count, dtype=jnp.int32)[:, None]
        - LEFT * SEG
        + jnp.arange(width, dtype=jnp.int32)[None, :]
    )
    allowed = (key_pos >= 0)[:, None, None, :] & (
        doc_band[:, None, None, :] == own_docs.reshape(count, SEG)[:, None, :, None]
    )
    scores = jnp.where(allowed, scores, -1e30)
    peak = jnp.max(scores, axis=-1, keepdims=True)
    expo = jnp.exp(scores - peak)
    weights = (expo / jnp.sum(expo, axis=-1, keepdims=True)).astype(jnp.bfloat16)
    mixed = jnp.zeros((count, SEG, heads_here, head_size), jnp.float32)
    for earlier in range(LEFT + 1):
        part_weights = weights[..., earlier * SEG : (earlier + 1) * SEG]
        mixed = mixed + jnp.einsum(
            "nhqk,nkhd->nqhd",
            part_weights,
            value_blocks[earlier : earlier + count],
            preferred_element_type=jnp.float32,
        )
    return mixed.astype(jnp.bfloat16).reshape(rows, heads_here * head_size)


def on_device(
    stream,
    doc_ids,
    norm_gain,
    query_weight,
    key_weight,
    value_weight,
    out_weight,
    query_gain,
    key_gain,
    rel_bias,
):
    rows = stream.shape[0]
    heads_here = rel_bias.shape[0]
    head_size = query_gain.shape[1]
    local_width = heads_here * head_size
    reach = LEFT * SEG
    depth = -(-reach // rows)
    offset = lax.axis_index("sp") * rows
    col_width = out_weight.shape[2]
    col_start = lax.axis_index("tp") * col_width
    table = bias_table(rel_bias)
    x = stream
    for layer in range(LAYERS):
        widened = x.astype(jnp.float32)
        normed = row_norm(widened, norm_gain[layer]).astype(jnp.bfloat16)
        own_cols = normed
        q_raw = jnp.dot(
            own_cols,
            lax.all_gather(query_weight[layer], "sp", axis=0, tiled=True),
            preferred_element_type=jnp.float32,
        )
        k_raw = jnp.dot(
            normed,
            lax.all_gather(key_weight[layer], "sp", axis=0, tiled=True),
            preferred_element_type=jnp.float32,
        )
        v_raw = jnp.dot(
            normed,
            lax.all_gather(value_weight[layer], "sp", axis=0, tiled=True),
            preferred_element_type=jnp.float32,
        )
        query = row_norm(q_raw.reshape(rows, heads_here, head_size), query_gain[layer]).astype(
            jnp.bfloat16
        )
        keys = row_norm(
            k_raw.reshape(normed.shape[0], heads_here, head_size), key_gain[layer]
        ).astype(jnp.bfloat16)
        values = v_raw.astype(jnp.bfloat16)
        flat_keys = keys.reshape(rows, local_width)
        tail = (flat_keys, values, doc_ids)
        received = [
            shifted((tail[0], tail[1], tail[2]), "sp", distance_back)
            for distance_back in range(depth, 0, -1)
        ]
        ext_keys = jnp.concatenate([item[0] for item in received] + [flat_keys], axis=0)
        ext_values = jnp.concatenate([item[1] for item in received] + [values], axis=0)
        ext_docs = jnp.concatenate([item[2] for item in received] + [doc_ids], axis=0)
        ext_keys = ext_keys.reshape(reach + rows, heads_here, head_size)
        ext_values = ext_values.reshape(reach + rows, heads_here, head_size)
        attended = attend(query, ext_keys, ext_values, ext_docs, doc_ids, offset, table)
        all_heads = lax.all_gather(attended, "tp", axis=1, tiled=True)
        projected = jnp.dot(
            all_heads,
            lax.all_gather(out_weight[layer], "sp", axis=0, tiled=True),
            preferred_element_type=jnp.float32,
        )
        own_cols = lax.dynamic_slice_in_dim(widened, col_start, col_width, 1)
        new_cols = (own_cols + projected).astype(jnp.bfloat16)
        x = lax.all_gather(new_cols, "tp", axis=1, tiled=True)
    return x


MESH = pl.DeviceIdType.MESH
NEG = -1e30


def fused_kernel(
    sizes,
    x_in,
    docs_ref,
    ngain_ref,
    qw_in,
    kw_in,
    vw_in,
    wo_in,
    qgain_ref,
    kgain_ref,
    bias_ref,
    out_ref,
    x_ref,
    qw_ref,
    kw_ref,
    vw_ref,
    woin_ref,
    load,
    save,
    wt_ref,
    xg,
    wq,
    wo,
    docs,
    dcol,
    mids,
    ag,
    fin,
    bias,
    masked,
    nb,
    q_s,
    k_s,
    v_s,
    o_s,
    doc_send,
    doc_recv,
    xz_send,
    xz_recv,
    xt_send,
    xt_recv,
    wz_send,
    wz_recv,
    wy_send,
    wy_recv,
    oz_send,
    oz_recv,
    ox_send,
    ox_recv,
    oy_send,
    oy_recv,
    op_send,
    op_recv,
    mz_send,
    mz_recv,
    mx_send,
    mx_recv,
    mc_send,
    mc_recv,
    nc_send,
    nc_recv,
    rs_send,
    rs_recv,
    az_send,
    az_recv,
    at_send,
    at_recv,
    fn_send,
    fn_recv,
):
    groups, seqs, tps = sizes
    rows, width = x_ref.shape
    cols = width // tps
    head = qgain_ref.shape[1]
    layers = wt_ref.shape[0]
    depth = bias.shape[1] - 1
    parts = xz_send.shape[1]
    tall = rows // parts
    pair = bias.shape[0]
    grp = lax.axis_index("grp")
    s = lax.axis_index("sp")
    t = lax.axis_index("tp")
    other_grp = 1 - grp
    core = t + 1 - 2 * lax.rem(t, 2)
    side = lax.rem(t + 2, tps)
    inner = (s > 0) & (s < seqs - 1)
    near = jnp.clip(s, 1, seqs - 2)
    far = seqs - 1 - near
    first = jnp.where(inner, seqs - 1 - s, near)
    inside = near - 1
    edge = jnp.where(near == 1, 0, seqs - 1)
    beyond = seqs - 1 - edge
    started = []

    def remote(src, dst, sems, out_index, in_index, where):
        return pltpu.make_async_remote_copy(
            src_ref=src,
            dst_ref=dst,
            send_sem=sems[0].at[out_index],
            recv_sem=sems[1].at[in_index],
            device_id=where,
            device_id_type=MESH,
        )

    def send(src, dst, sems, index, where):
        copy = remote(src, dst, sems, index, index, where)
        copy.start()
        started.append(copy)
        return copy

    def settle():
        for copy in started:
            copy.wait_send()
        started.clear()

    def ahead(o):
        return lax.rem(s + o, seqs)

    def block_rows(i):
        return pl.ds(pl.multiple_of(i * rows, rows), rows)

    def cut_rows(i, h):
        return pl.ds(pl.multiple_of(i * rows + h * tall, tall), tall)

    loads = [
        pltpu.make_async_copy(src, dst, load.at[n])
        for n, (src, dst) in enumerate(
            zip((x_in, qw_in, kw_in, vw_in, wo_in), (x_ref, qw_ref, kw_ref, vw_ref, woin_ref))
        )
    ]
    for copy in loads:
        copy.start()
    barrier = pltpu.get_barrier_semaphore()
    partners = [{"sp": ahead(o)} for o in range(1, seqs)]
    partners += [{"tp": core}, {"tp": side}, {"grp": other_grp}]
    for where in partners:
        pl.semaphore_signal(barrier, inc=1, device_id=where, device_id_type=MESH)
    pl.semaphore_wait(barrier, len(partners))
    loads[0].wait()

    own_cols = pl.ds(pl.multiple_of(t * cols, cols), cols)
    ohalf = woin_ref.shape[1] // 2
    opart = pl.ds(pl.multiple_of(grp * ohalf, ohalf), ohalf)
    hops = list(range(1, seqs))

    def x_copy(source, dest, h):
        place = xg.at[0, t, cut_rows(source, h), :]
        return remote(
            x_ref.at[h * tall : (h + 1) * tall, own_cols],
            place,
            (xz_send, xz_recv),
            (dest, h),
            (source, h),
            {"sp": dest},
        )

    def w_copy(layer, source, dest):
        return remote(
            wt_ref.at[layer, pair * (dest - 1) + grp],
            wq.at[layer, source, grp],
            (wz_send, wz_recv),
            (layer, dest),
            (layer, source),
            {"sp": dest},
        )

    def o_copy(layer, source, dest):
        return remote(
            woin_ref.at[layer, opart, :],
            wo.at[layer, t, source, opart, :],
            (oz_send, oz_recv),
            (layer, dest),
            (layer, source),
            {"sp": dest},
        )

    def w_full(layer, source, dest):
        return remote(
            wt_ref.at[layer, pl.ds(pair * (dest - 1), pair)],
            wq.at[layer, source],
            (wz_send, wz_recv),
            (layer, dest),
            (layer, source),
            {"sp": dest},
        )

    def o_full(layer, source, dest):
        return remote(
            woin_ref.at[layer],
            wo.at[layer, t, source],
            (oz_send, oz_recv),
            (layer, dest),
            (layer, source),
            {"sp": dest},
        )

    def outer_plan(n):
        if n == 0:
            return [x_copy(s, near, h) for h in range(parts)]
        if n == 1:
            x_far = [x_copy(s, far, h) for h in range(parts)]
            return [w_copy(0, s, near)] + x_far + [w_copy(0, s, far)]
        if n == 2:
            return [o_copy(0, s, far), o_full(0, s, near)]
        plan = [w_copy(1, s, near), w_copy(1, s, far)]
        return plan + [o_copy(1, s, far), o_full(1, s, near), o_copy(1, s, seqs - 1 - s)]

    def inner_plan(n):
        other = seqs - 1 - s
        if n == 0:
            return [x_copy(s, other, h) for h in range(parts)]
        if n == 1:
            return [w_copy(0, s, other), o_full(1, s, edge)]
        if n == 2:
            return [o_copy(0, s, other), w_copy(1, s, other)]
        return [o_copy(1, s, other), o_copy(1, s, beyond)]

    def sends(plan, n, act):
        for copy in plan(n):
            getattr(copy, act)()

    def tp_copy(kind, block, h):
        held = side if kind == 2 else t
        place = xg.at[0, held, cut_rows(block, h), :]
        index = (kind, block, h)
        where = {"tp": side if kind == 1 else core}
        return remote(place, place, (xt_send, xt_recv), index, index, where)

    def w_relay(layer, block):
        place = wq.at[layer, block, grp]
        index = (layer, block)
        return remote(place, place, (wy_send, wy_recv), index, index, {"grp": other_grp})

    def o_relay(layer, kind, block):
        held = side if kind == 2 else t
        place = wo.at[layer, held, block, opart, :]
        sems = ((ox_send, ox_recv), (oy_send, oy_recv), (op_send, op_recv))[kind]
        index = (layer, block)
        where = {"tp": side} if kind == 0 else {"grp": other_grp}
        return remote(place, place, sems, index, index, where)

    def o_whole(layer):
        place = wo.at[layer, t, s]
        index = (layer, s)
        return remote(woin_ref.at[layer], place, (ox_send, ox_recv), index, index, {"tp": side})

    def begin(copy):
        copy.start()
        started.append(copy)

    def fan(block, h):
        x_copy(block, near, h).wait_recv()
        begin(tp_copy(1, block, h))
        begin(tp_copy(0, block, h))

    def pass_on(block, h):
        tp_copy(1, block, h).wait_recv()
        begin(tp_copy(2, block, h))

    def spread_w(layer, block):
        w_copy(layer, block, near).wait_recv()
        begin(w_relay(layer, block))

    def spread_o(layer, block, whole=False):
        (o_full(layer, block, near) if whole else o_copy(layer, block, near)).wait_recv()
        begin(o_relay(layer, 0, block))
        if not whole:
            begin(o_relay(layer, 1, block))

    def side_o(layer, block):
        o_relay(layer, 0, block).wait_recv()
        begin(o_relay(layer, 2, block))

    def ready_own(layer, relayed):
        for block in relayed:
            o_relay(layer, 1, block).wait_recv()

    def ready_side(layer, sides):
        o_whole(layer).wait_recv()
        for block in sides:
            o_relay(layer, 2, block).wait_recv()

    def ready_o(layer, relayed, sides):
        ready_own(layer, relayed)
        ready_side(layer, sides)

    def turn(layer):
        for which, source in enumerate((qw_ref, kw_ref, vw_ref)):
            turned = jnp.transpose(source[layer])
            for i in range(seqs):
                wt_ref[layer, i, which * head : (which + 1) * head, :] = turned[
                    i * head : (i + 1) * head, :
                ]

    @pl.when(inner)
    def _():
        sends(inner_plan, 0, "start")

    @pl.when(jnp.logical_not(inner))
    def _():
        sends(outer_plan, 0, "start")

    docs[s] = jnp.broadcast_to(docs_ref[...].astype(jnp.float32), docs.shape[1:])
    doc_c = [
        remote(docs.at[s], docs.at[s], (doc_send, doc_recv), o, o, {"sp": ahead(o)}) for o in hops
    ]
    for copy in doc_c:
        copy.start()
    for copy in loads[1:]:
        copy.wait()
    turn(0)

    @pl.when(inner)
    def _():
        sends(inner_plan, 1, "start")

    @pl.when(jnp.logical_not(inner))
    def _():
        for n in (1, 2):
            sends(outer_plan, n, "start")

    for layer in range(1, layers):
        turn(layer)

    @pl.when(jnp.logical_not(inner))
    def _():
        sends(outer_plan, 3, "start")

    for layer in range(layers):
        wo[layer, t, s] = woin_ref[layer]
    assert not started

    def project(layer, i):
        total = jnp.zeros((rows, 1), jnp.float32)
        for part in range(tps):
            piece = xg[layer, part, block_rows(i), :].astype(jnp.float32)
            total = total + jnp.sum(piece * piece, axis=1, keepdims=True)
        factor = lax.rsqrt(total * (1.0 / width) + epsilon)
        for part in range(tps):
            piece = xg[layer, part, block_rows(i), :].astype(jnp.float32)
            gain = ngain_ref[layer : layer + 1, part * cols : (part + 1) * cols]
            nb[:, part * cols : (part + 1) * cols] = (piece * factor * gain).astype(jnp.bfloat16)
        span = width // seqs
        raw = jnp.zeros((pair * 3 * head, rows), jnp.float32)
        for part in range(seqs):
            raw = raw + lax.dot_general(
                wq[layer, part].reshape(pair * 3 * head, span),
                nb[:, part * span : (part + 1) * span],
                (((1,), (1,)), ((), ())),
                preferred_element_type=jnp.float32,
            )

        def normal(value, gain):
            mean = jnp.mean(value * value, axis=0, keepdims=True)
            column = jnp.transpose(jnp.broadcast_to(gain, (128, head)))[:, 0:1]
            return value * lax.rsqrt(mean + epsilon) * column

        for a in range(pair):
            query, keys, values = [
                raw[(3 * a + n) * head : (3 * a + n + 1) * head] for n in range(3)
            ]
            query = normal(query, qgain_ref[layer : layer + 1, :]) * head ** (-0.5)
            keys = normal(keys, kgain_ref[layer : layer + 1, :])
            q_s[a, i] = query.astype(jnp.bfloat16)
            k_s[a, i] = jnp.transpose(keys).astype(jnp.bfloat16)
            v_s[a, i] = values.astype(jnp.bfloat16)

    links = [(i, j) for j in range(seqs) for i in range(max(0, j - depth), j + 1)]

    def mask(a):
        for n, (i, j) in enumerate(links):
            same = dcol[i][:, 0:1] == docs[j, 0:1, :]
            masked[a, n] = jnp.where(same, bias[a, j - i], NEG)

    def attend_block(j, a):
        pieces = []
        for i in range(max(0, j - depth), j + 1):
            score = jnp.dot(k_s[a, i], q_s[a, j], preferred_element_type=jnp.float32)
            pieces.append((i, score + masked[a, links.index((i, j))]))
        peak = pieces[0][1].max(axis=0, keepdims=True)
        for _, piece in pieces[1:]:
            peak = jnp.maximum(peak, piece.max(axis=0, keepdims=True))
        mass = jnp.zeros((1, rows), jnp.float32)
        mixed = jnp.zeros((head, rows), jnp.float32)
        for i, piece in pieces:
            expo = jnp.exp(piece - peak)
            mass = mass + jnp.sum(expo, axis=0, keepdims=True)
            mixed = mixed + jnp.dot(
                v_s[a, i], expo.astype(jnp.bfloat16), preferred_element_type=jnp.float32
            )
        return (mixed / mass).astype(jnp.bfloat16)

    def out_product(layer, heads_all, held):
        return lax.dot_general(
            heads_all,
            wo[layer, held].reshape(-1, cols),
            (((0,), (0,)), ((), ())),
            preferred_element_type=jnp.float32,
        )

    def rest_copy(half, held):
        place = xg.at[1, held, block_rows(edge), :]
        return remote(place, place, (rs_send, rs_recv), half, half, {"sp": edge})

    def ag_copy(kind, n):
        place = ag.at[side if kind else t, n]
        index = (kind, n)
        where = {"tp": core if kind else side}
        return remote(place, place, (at_send, at_recv), index, index, where)

    def beside_copy():
        place = ag.at[t]
        return remote(place, place, (at_send, at_recv), (2, 0), (2, 0), {"tp": core})

    def last_copy(j):
        return remote(
            o_s.at[j], ag.at[t, inside], (az_send, az_recv), j, inside, {"sp": j}
        )

    @pl.when(inner)
    def _():
        other = seqs - 1 - s
        for part in range(tps):
            xg[0, part, block_rows(s), :] = x_ref[:, part * cols : (part + 1) * cols]
        for layer in range(layers):
            wq[layer, s] = wt_ref[layer, pl.ds(pair * inside, pair)]
        begin(o_whole(0))
        key_seg = lax.broadcasted_iota(jnp.int32, (rows, rows), 0) // SEG
        query_seg = lax.broadcasted_iota(jnp.int32, (rows, rows), 1) // SEG
        entries = (bias_ref.shape[1] - 1) // 128 * 128
        tables = []
        for a in range(pair):
            line = bias_ref[pl.ds(pair * inside + a, 1), :]
            line, final = line[:, :entries], line[:, entries:]
            tables.append(
                jnp.concatenate(
                    [line, jnp.broadcast_to(final, (1, (depth + 2) * rows - entries))], axis=1
                )
            )
        for d in range(depth + 1):
            gap = query_seg + (d * rows) // SEG - key_seg
            for a in range(pair):
                spread = jnp.broadcast_to(
                    tables[a][:, d * rows : (d + 2) * rows], (rows, 2 * rows)
                )
                rolled = pltpu.roll(spread, 0, 1, stride=1, stride_axis=0)
                bias[a, d] = jnp.where((gap >= 0) & (gap <= LEFT), rolled[:, rows:], NEG)
        order = [(block, h) for h in range(parts) for block in (edge, other)]
        fan(*order[0])
        fan(*order[1])
        for copy in doc_c:
            copy.wait_recv()
        for i in range(seqs):
            dcol[i] = jnp.transpose(jnp.broadcast_to(docs[i, 0:1, :], (128, rows)))
        mask(0)
        pass_on(*order[0])
        fan(*order[2])
        fan(*order[3])
        pass_on(*order[1])
        spread_w(0, edge)
        spread_w(0, other)
        mask(1)
        pass_on(*order[2])
        fan(beyond, 0)
        pass_on(*order[3])
        spread_w(0, beyond)
        sends(inner_plan, 2, "start")
        for h in range(1, parts):
            fan(beyond, h)
        pass_on(beyond, 0)
        for h in range(1, parts):
            pass_on(beyond, h)
        for block in (edge, other, beyond):
            w_relay(0, block).wait_recv()
        project(0, s)
        spread_o(0, other)
        for block in (edge, other, beyond):
            for h in range(parts):
                tp_copy(0, block, h).wait_recv()
                tp_copy(2, block, h).wait_recv()
            project(0, block)
            if block is edge:
                spread_o(0, edge, True)
            if block is other:
                spread_o(0, beyond)

        mid_z, mid_x, mid_c, new_c = {}, {}, {}, {}
        turns = (0, 3, 1, 2)
        for n, j in enumerate(turns):
            for a in range(pair):
                mids[j, t, inside, a * head : (a + 1) * head, :] = attend_block(j, a)
            place = mids.at[j, t, inside]
            mid_z[j] = send(place, place, (mz_send, mz_recv), j, {"sp": other})
            mid_x[j, 0] = send(place, place, (mx_send, mx_recv), (j, 0), {"tp": side})
            if n == 0:
                side_o(0, other)
            if n == 1:
                side_o(0, edge)
            if n == 2:
                spread_w(1, other)

        def mid_first(j):
            mid_z[j].wait_recv()
            place = mids.at[j, t, 1 - inside]
            mid_x[j, 1] = send(place, place, (mx_send, mx_recv), (j, 1), {"tp": side})
            place = mids.at[j, t]
            mid_c[j, 0] = send(place, place, (mc_send, mc_recv), (j, 0), {"tp": core})

        def mid_second(j):
            for n in range(2):
                mid_x[j, n].wait_recv()
            place = mids.at[j, side]
            mid_c[j, 1] = send(place, place, (mc_send, mc_recv), (j, 1), {"tp": core})

        def mid_third(j, half):
            if half == 0:
                for n in range(2):
                    mid_c[j, n].wait_recv()
            held = side if half else t
            heads_all = mids[j].reshape(tps * seqs * head, rows)
            kept = xg[0, held, block_rows(j), :].astype(jnp.float32)
            place = xg.at[1, held, block_rows(j), :]
            place[...] = (kept + out_product(0, heads_all, held)).astype(jnp.bfloat16)
            new_c[j, half] = send(place, place, (nc_send, nc_recv), (j, half), {"tp": core})
            if j in (0, seqs - 1):

                @pl.when(edge == j)
                def _():
                    rest_copy(half, held).start()

        def mid_fourth(j):
            for half in range(2):
                new_c[j, half].wait_recv()
            project(1, j)

        mid_first(0)
        side_o(0, beyond)
        mid_first(3)
        mid_second(0)
        spread_w(1, beyond)
        mid_first(1)
        mid_second(3)
        mid_first(2)
        mid_second(1)
        mid_second(2)
        spread_w(1, edge)
        begin(o_whole(1))
        sends(inner_plan, 3, "start")
        ready_own(0, (other, beyond))
        mid_third(0, 0)
        mid_third(3, 0)
        mid_third(1, 0)
        ready_side(0, (edge, other, beyond))
        mid_third(0, 1)
        mid_third(3, 1)
        spread_o(1, beyond)
        mid_third(1, 1)
        w_relay(1, edge).wait_recv()
        for block in (other, beyond):
            w_relay(1, block).wait_recv()
        def finish(j):
            for a in range(pair):
                o_s[j, a * head : (a + 1) * head, :] = attend_block(j, a)

            @pl.when(s != j)
            def _():
                last_copy(j).start()

        mid_third(2, 0)
        mid_third(2, 1)
        mid_fourth(0)
        finish(0)
        spread_o(1, other)
        mid_fourth(3)
        spread_o(1, edge, True)
        side_o(1, beyond)
        mid_fourth(1)
        finish(1)
        side_o(1, other)
        mid_fourth(2)
        finish(3)
        side_o(1, edge)
        finish(2)
        ag[t, inside] = o_s[s]
        begin(ag_copy(0, inside))
        ag_in = remote(o_s.at[0], ag.at[t, 1 - inside], (az_send, az_recv), s, 1 - inside, {"sp": other})
        ag_in.wait_recv()
        begin(ag_copy(0, 1 - inside))
        begin(beside_copy())
        ready_o(1, (other, beyond), (edge, other, beyond))
        for half, held in enumerate((t, side)):
            rest_copy(half, held).wait_send()
        for o in hops:
            last_copy(ahead(o)).wait_send()
        for n in range(4):
            sends(inner_plan, n, "wait_send")
        settle()

    @pl.when(jnp.logical_not(inner))
    def _():
        begin(o_whole(1))
        for copy in doc_c:
            copy.wait_recv()
        spread_o(1, near, True)
        for block in (seqs - 1 - s, far):
            spread_o(1, block)
        for o in hops:
            side_o(1, ahead(o))
        for half, held in enumerate((t, side)):
            rest_copy(half, held).wait_recv()
        for n in (inside, 1 - inside):
            place = ag.at[t, n]
            remote(place, place, (az_send, az_recv), s, n, {"sp": near}).wait_recv()
            begin(ag_copy(0, n))
        begin(beside_copy())
        ready_o(1, (far, seqs - 1 - s), (near, far, seqs - 1 - s))
        settle()
        for n in range(4):
            sends(outer_plan, n, "wait_send")

    for n in (inside, 1 - inside):
        ag_copy(0, n).wait_recv()
        begin(ag_copy(1, n))
    beside_copy().wait_recv()
    for n in (inside, 1 - inside):
        ag_copy(1, n).wait_recv()
    heads_all = ag[...].reshape(tps * seqs * head, rows)
    last, stores = [], []

    def store(part):
        place = out_ref.at[:, pl.ds(pl.multiple_of(part * cols, cols), cols)]
        return pltpu.make_async_copy(fin.at[part], place, save.at[part])

    for half, held in enumerate((t, side)):
        kept = xg[1, held, block_rows(s), :].astype(jnp.float32)
        fin[held] = (kept + out_product(1, heads_all, held)).astype(jnp.bfloat16)
        place = fin.at[held]
        last.append(send(place, place, (fn_send, fn_recv), half, {"tp": core}))
        stores.append(store(held))
        stores[-1].start()
    for copy, held in zip(last, (core, lax.rem(core + 2, tps))):
        copy.wait_recv()
        stores.append(store(held))
        stores[-1].start()
    settle()
    for copy in doc_c:
        copy.wait_send()
    for copy in stores:
        copy.wait()

def fused_device(
    sizes,
    stream,
    doc_ids,
    norm_gain,
    query_weight,
    key_weight,
    value_weight,
    out_weight,
    query_gain,
    key_gain,
    rel_bias,
):
    groups, seqs, tps = sizes
    rows, width = stream.shape
    cols = width // tps
    layers, deep, _ = query_weight.shape
    head = query_gain.shape[1]
    depth = -(-LEFT * SEG // rows)

    dma = pltpu.SemaphoreType.DMA
    bf16 = jnp.bfloat16
    pair = seqs // 2
    links = sum(min(j, depth) + 1 for j in range(seqs))
    whole = [stream, query_weight, key_weight, value_weight, out_weight]
    scratch = [pltpu.VMEM(one.shape, one.dtype) for one in whole] + [dma((len(whole),)), dma((tps,))]
    scratch += [
        pltpu.VMEM((layers, seqs, 3 * head, deep), bf16),
        pltpu.VMEM((layers, tps, seqs * rows, cols), bf16),
        pltpu.VMEM((layers, seqs, pair, 3 * head, deep), bf16),
        pltpu.VMEM((layers, tps, seqs) + out_weight.shape[1:], bf16),
        pltpu.VMEM((seqs, 8, rows), jnp.float32),
        pltpu.VMEM((seqs, rows, 128), jnp.float32),
        pltpu.VMEM((seqs, tps, 2, pair * head, rows), bf16),
        pltpu.VMEM((tps, 2, pair * head, rows), bf16),
        pltpu.VMEM((tps, rows, cols), bf16),
        pltpu.VMEM((pair, depth + 1, rows, rows), jnp.float32),
        pltpu.VMEM((pair, links, rows, rows), jnp.float32),
        pltpu.VMEM((rows, width), bf16),
        pltpu.VMEM((pair, seqs, head, rows), bf16),
        pltpu.VMEM((pair, seqs, rows, head), bf16),
        pltpu.VMEM((pair, seqs, head, rows), bf16),
        pltpu.VMEM((seqs, pair * head, rows), bf16),
    ]
    pairs = [
        (seqs,),
        (seqs, 2),
        (3, seqs, 2),
        (layers, seqs),
        (layers, seqs),
        (layers, seqs),
        (layers, seqs),
        (layers, seqs),
        (layers, seqs),
        (seqs,),
        (seqs, 2),
        (seqs, 2),
        (seqs, 2),
        (2,),
        (seqs,),
        (3, 2),
        (2,),
    ]
    scratch += [dma(shape) for shape in pairs for _ in range(2)]
    return pl.pallas_call(
        functools.partial(fused_kernel, sizes),
        name="fused_layers",
        out_shape=jax.ShapeDtypeStruct((rows, width), bf16),
        in_specs=[
            pl.BlockSpec(memory_space=pltpu.HBM if n in (0, 3, 4, 5, 6) else pltpu.VMEM)
            for n in range(10)
        ],
        out_specs=pl.BlockSpec(memory_space=pl.ANY),
        scratch_shapes=scratch,
        compiler_params=pltpu.CompilerParams(
            collective_id=0, has_side_effects=True, vmem_limit_bytes=58 * 1024 * 1024
        ),
    )(
        stream,
        doc_ids[None],
        norm_gain,
        query_weight,
        key_weight,
        value_weight,
        out_weight,
        query_gain,
        key_gain,
        rel_bias,
    )


def solution(mesh):
    placed = (
        P(("grp", "sp"), None),
        P(("grp", "sp")),
        P(),
        P(None, "sp", "tp"),
        P(None, "sp", "tp"),
        P(None, "sp", "tp"),
        P(None, "sp", "tp"),
        P(),
        P(),
        P("tp", None),
    )
    sizes = tuple(mesh.shape[axis] for axis in ("grp", "sp", "tp"))

    def body(*args):
        one_head_each = args[-1].shape[0] == sizes[1]
        fits = sizes == (2, 4, 4) and args[0].shape[0] == MAXREL
        if one_head_each and fits:
            return fused_device(sizes, *args)
        return on_device(*args)

    return jax.shard_map(
        body, mesh=mesh, in_specs=placed, out_specs=P(("grp", "sp"), None), check_vma=False
    )
```
